32 devices in a mesh: sp: 4 (over y, core), dp: 8 (over z, x).
Axes of the slice: x: 2, y: 2, z: 4, core: 2. Of those that a mesh axis runs over, the one named last changes fastest.
Arguments:
- queries: bfloat16 [8, 1024, 1024], P('dp', 'sp'), may hold values from -250 to 250
- keys: bfloat16 [8, 1024, 1024], P('dp', 'sp'), may hold values from -6 to 6
- values: bfloat16 [8, 1024, 1024], P('dp', 'sp'), may hold values from -6 to 6
- cum_gate: float32 [8, 16, 1024], P('dp', 'sp'), may hold values from -1024 to 0, as said below
- out_weight: bfloat16 [1024, 2112], P(None, 'dp'), may hold values from -1.5 to 1.5
Outputs:
- mixed: bfloat16 [8, 1024, 2112], P('dp', 'sp')
The draws below stay inside these ranges and needn't reach their ends.
Inputs may be any that keep to these rules, and one draw needn't show every extreme that they name: `cum_gate`: within each head the entries do not rise along positions.
All inputs are finite; a program needn't handle non-finite values.
Results may differ from the reference program's by a relative error of at most 0.0053.
Values may be sent and summed in bfloat16 or wider, within the bound.
A program may use at most 64 MiB of HBM per device.

```python
import jax
import jax.numpy as jnp
from jax import lax

D = 2112
HEAD_COUNT = 16
HEAD_DIM = 64
TOK_DEV = 256
WIDTH = 1024
SEQUENCE_LENGTH = 1024
SEQUENCE_COUNT = 8


def drawn_pair(key):
    key_query, key_key = jax.random.split(jax.random.fold_in(key, 11), 2)
    query_draw = 1.5 * jnp.clip(jax.random.normal(key_query, (SEQUENCE_COUNT, SEQUENCE_LENGTH, WIDTH), jnp.float32), -6.0, 6.0)
    key_draw = jnp.clip(jax.random.normal(key_key, (SEQUENCE_COUNT, SEQUENCE_LENGTH, WIDTH), jnp.float32), -6.0, 6.0)
    return (query_draw, key_draw)


def draw_queries(key, part):
    return drawn_pair(key)[0].astype(jnp.bfloat16)


def draw_keys(key, part):
    return drawn_pair(key)[1].astype(jnp.bfloat16)


def draw_values(key, part):
    base = jax.random.normal(jax.random.fold_in(key, 31), (SEQUENCE_COUNT, SEQUENCE_LENGTH, WIDTH), jnp.float32)
    return jnp.clip(base, -6.0, 6.0).astype(jnp.bfloat16)


def draw_cum_gate(key, part):
    key_heads, key_slow, key_fast, key_block, key_rough, key_place, key_loss = jax.random.split(jax.random.fold_in(key, 23), 7)
    head_order = jax.random.permutation(key_heads, HEAD_COUNT)
    sluggish_head = head_order < HEAD_COUNT // 2
    sluggish_head = sluggish_head[None, :, None]
    slow_rate = jax.random.uniform(key_slow, (SEQUENCE_COUNT, HEAD_COUNT, 1), jnp.float32, 0.3, 1.0) / SEQUENCE_LENGTH
    fast_rate = jax.random.uniform(key_fast, (SEQUENCE_COUNT, HEAD_COUNT, 1), jnp.float32, 1.0 / 100.0, 1.0 / 30.0)
    baseline_decay = jnp.where(sluggish_head, slow_rate, fast_rate)
    shard_count = SEQUENCE_LENGTH // TOK_DEV
    block_multiplier = jnp.exp(jax.random.uniform(key_block, (SEQUENCE_COUNT, HEAD_COUNT, shard_count, 1), jnp.float32, jnp.log(0.5), jnp.log(2.0)))
    block_multiplier = jnp.broadcast_to(block_multiplier, (SEQUENCE_COUNT, HEAD_COUNT, shard_count, TOK_DEV)).reshape(SEQUENCE_COUNT, HEAD_COUNT, SEQUENCE_LENGTH)
    jitter_level = jax.random.uniform(key_rough, (SEQUENCE_COUNT, HEAD_COUNT, SEQUENCE_LENGTH), jnp.float32, 0.3, 1.7)
    spike_locations = jax.random.randint(key_place, (SEQUENCE_COUNT, HEAD_COUNT, 3), 0, SEQUENCE_LENGTH)
    decay_amounts = jax.random.uniform(key_loss, (SEQUENCE_COUNT, HEAD_COUNT, 3), jnp.float32, 0.22, 0.5)
    token_positions = jnp.arange(SEQUENCE_LENGTH, dtype=jnp.int32)
    spike_events = jnp.zeros((SEQUENCE_COUNT, HEAD_COUNT, SEQUENCE_LENGTH), jnp.float32)
    for spike_event in range(3):
        spike_events = spike_events + jnp.where(token_positions[None, None, :] == spike_locations[:, :, spike_event:spike_event + 1], decay_amounts[:, :, spike_event:spike_event + 1], 0.0)
    gate_logarithm = -baseline_decay * block_multiplier * jitter_level - jnp.where(sluggish_head, spike_events, 0.0)
    return jnp.cumsum(gate_logarithm, axis=-1)


def levels(stream_key, shape, cuts, low, top_value):
    loudness = 1.0
    for dim, blocks in cuts:
        steps = jax.random.uniform(jax.random.fold_in(jax.random.fold_in(stream_key, 6), dim), (blocks,), jnp.float32, low / len(cuts), top_value / len(cuts))
        loudness = loudness * jnp.repeat(jnp.exp(steps), shape[dim] // blocks).reshape((-1,) + (1,) * (len(shape) - 1 - dim))
    return loudness


def normal_values(key, dims, scale, most, shards=(), kind=jnp.bfloat16):
    array = scale * jax.random.normal(key, dims, jnp.float32)
    if shards:
        array = array * levels(key, dims, shards, -0.22, 0.18)
    return jnp.clip(array, -most, most).astype(kind)


def setup_inputs(seed: int = 0) -> dict:
    key_list = jax.random.split(jax.random.key(seed), 6)
    queries = draw_queries(jax.random.fold_in(key_list[5], 71), 0)
    keys = draw_keys(jax.random.fold_in(key_list[5], 71), 0)
    values = draw_values(jax.random.fold_in(key_list[5], 71), 0)
    cum_gate = draw_cum_gate(jax.random.fold_in(key_list[5], 71), 0)
    out_weight = normal_values(key_list[4], (WIDTH, D), (WIDTH // 64) ** -0.5, 1.5, ((1, 8),))
    return {"queries": queries, "keys": keys, "values": values, "cum_gate": cum_gate, "out_weight": out_weight}


def reference(queries, keys, values, cum_gate, out_weight):
    sequences, length, width = queries.shape
    block_rows = min(512, length)
    block_count = length // block_rows
    score_scale = HEAD_DIM ** -0.5
    token_positions = jnp.arange(length, dtype=jnp.int32)

    def one_sequence(arrays):
        query_seq, key_seq, value_seq, gate_seq = arrays
        query_f = query_seq.astype(jnp.float32).reshape(length, HEAD_COUNT, HEAD_DIM)
        key_f = key_seq.astype(jnp.float32).reshape(length, HEAD_COUNT, HEAD_DIM)
        value_f = value_seq.astype(jnp.float32).reshape(length, HEAD_COUNT, HEAD_DIM)

        def one_block(block_index):
            first_row = (block_index * block_rows).astype(jnp.int32)
            query_part = lax.dynamic_slice_in_dim(query_f, first_row, block_rows, 0)
            gate_part = lax.dynamic_slice_in_dim(gate_seq, first_row, block_rows, 1)
            logits = jnp.einsum('qhe,khe->hqk', query_part, key_f) * score_scale
            logits = logits + gate_part[:, :, None] - gate_seq[:, None, :]
            query_rows = first_row + jnp.arange(block_rows, dtype=jnp.int32)
            allowed = token_positions[None, None, :] <= query_rows[None, :, None]
            logits = jnp.where(allowed, logits, -jnp.inf)
            scores = jnp.exp(logits - jnp.max(logits, axis=-1, keepdims=True))
            denominator = jnp.sum(scores, axis=-1)
            scores_low = lax.optimization_barrier(scores.astype(jnp.bfloat16)).astype(jnp.float32)
            weighted = jnp.einsum('hqk,khe->hqe', scores_low, value_f) / denominator[..., None]
            return weighted.transpose(1, 0, 2).reshape(block_rows, width).astype(jnp.bfloat16)

        blocks = lax.map(one_block, jnp.arange(block_count, dtype=jnp.int32))
        return blocks.reshape(length, width)

    attended = lax.map(one_sequence, (queries, keys, values, cum_gate))
    mixed = jnp.dot(attended.reshape(sequences * length, width), out_weight,
                    preferred_element_type=jnp.float32)
    return mixed.astype(jnp.bfloat16).reshape(sequences, length, out_weight.shape[1])
```

```python
import functools
import math

import jax
import jax.numpy as jnp
from jax import lax
from jax.experimental import pallas as pl
from jax.experimental.pallas import tpu as pltpu
from jax.sharding import PartitionSpec as P

LANES = 128
SUBLANES = 16
MESH = pl.DeviceIdType.MESH


def ring_index(position, n):
    upper = position // (n // 2)
    return (1 - upper) * (2 * position) + upper * (2 * (n - 1 - position) + 1)


def fused_kernel(
    sp, dp, depth, q, k, v, gate, w, out,
    qg, kg, vg, og, attended, wg,
    qkv_send, qkv_recv, qkv_local, out_send, out_recv, out_local,
    ring_send, ring_recv, pair_send, pair_recv, own_sem,
):
    tokens, width = q.shape
    group = width // sp
    pairs = group // LANES
    per_pair = LANES // depth
    half = width // 2
    columns = w.shape[0]
    steps = dp // 2
    cut = -(-(columns // 2) // SUBLANES) * SUBLANES
    me = lax.axis_index("sp")
    mine = lax.axis_index("dp")
    core = lax.rem(me, 2)
    partner = me + 1 - 2 * core
    odd = lax.rem(mine, 2)
    position = (1 - odd) * (mine // 2) + odd * (dp - 1 - mine // 2)
    right = ring_index(lax.rem(position + 1, dp), dp)
    left = ring_index(lax.rem(position + dp - 1, dp), dp)

    barrier = pltpu.get_barrier_semaphore()
    for d in range(1, sp):
        pl.semaphore_signal(
            barrier, inc=1, device_id=(lax.rem(me + d, sp), mine), device_id_type=MESH
        )
    for side in (left, right):
        pl.semaphore_signal(barrier, inc=1, device_id=(me, side), device_id_type=MESH)

    own_copies = [pltpu.make_async_copy(w, wg.at[mine], own_sem.at[0])]
    local_copies = {}
    arrays = ((q, qg), (k, kg), (v, vg))
    for p in range(pairs):
        for a, (source, target) in enumerate(arrays):
            local_copies[p, a] = pltpu.make_async_copy(
                source.at[:, pl.ds(pl.multiple_of(me * group + p * LANES, LANES), LANES)],
                target.at[p, pl.ds(pl.multiple_of(me * tokens, tokens), tokens), :],
                qkv_local.at[p, a])
    pl.semaphore_wait(barrier, sp + 1)

    qkv_copies = {}
    order = [2, 1, 3] if sp == 4 else list(range(1, sp))

    def send_pair(p):
        for a, (source, target) in enumerate(arrays):
            for d in order:
                peer = lax.rem(me + d, sp)
                copy = pltpu.make_async_remote_copy(
                    src_ref=source.at[:, pl.ds(pl.multiple_of(peer * group + p * LANES, LANES), LANES)],
                    dst_ref=target.at[p, pl.ds(pl.multiple_of(me * tokens, tokens), tokens), :],
                    send_sem=qkv_send.at[p, a, d - 1],
                    recv_sem=qkv_recv.at[p, a, d - 1],
                    device_id=(peer, mine),
                    device_id_type=MESH,
                )
                copy.start()
                qkv_copies[p, a, d] = copy

    ring_copies = {}
    pair_copies = {}

    lanes = pl.ds(pl.multiple_of(core * half, half), half)

    def ring_slice(owner, side, step):
        if step < steps - 1:
            return wg.at[owner, :, lanes]
        if side == 0:
            return wg.at[owner, pl.ds(0, cut), lanes]
        return wg.at[owner, pl.ds(cut, columns - cut), lanes]

    def start_ring(key, source, target, side, slot):
        copy = pltpu.make_async_remote_copy(
            src_ref=source, dst_ref=target,
            send_sem=ring_send.at[side, slot], recv_sem=ring_recv.at[side, slot],
            device_id=(me, right if side == 0 else left), device_id_type=MESH)
        copy.start()
        ring_copies[key] = copy

    def ring_first():
        for side in range(2):
            start_ring((side, 0), w.at[:, lanes], wg.at[mine, :, lanes], side, 0)

    def ring_step(step):
        for side in range(2):
            ring_copies[side, step].wait_recv()
            shift = dp - 1 - step if side == 0 else 1 + step
            owner = ring_index(lax.rem(position + shift, dp), dp)
            if step + 1 < steps:
                piece = ring_slice(owner, side, step + 1)
                start_ring((side, step + 1), piece, piece, side, step + 1)
            piece = ring_slice(owner, side, step)
            copy = pltpu.make_async_remote_copy(
                src_ref=piece, dst_ref=piece,
                send_sem=pair_send.at[side, step], recv_sem=pair_recv.at[side, step],
                device_id=(partner, mine), device_id_type=MESH)
            copy.start()
            pair_copies[side, step] = copy

    send_pair(0)
    ring_first()
    for p in range(1, pairs):
        send_pair(p)
    for copy in local_copies.values():
        copy.start()
    for copy in own_copies:
        copy.start()

    log2e = math.log2(math.e)
    factor = depth ** -0.5 * log2e
    gates = gate[...] * log2e
    gates_t = jnp.transpose(gates)
    lane = lax.broadcasted_iota(jnp.int32, (tokens, LANES), 1) // depth
    diagonal = (
        lax.broadcasted_iota(jnp.int32, (tokens, tokens), 1)
        <= lax.broadcasted_iota(jnp.int32, (tokens, tokens), 0)
    )

    def attend_block(p, i):
        keys = (i + 1) * tokens
        query = qg[p, i * tokens:keys, :]
        key = kg[p, 0:keys, :]
        value = vg[p, 0:keys, :]
        result = jnp.zeros((tokens, LANES), jnp.float32)
        for j in range(per_pair):
            h = p * per_pair + j
            masked = jnp.where(lane == j, query, jnp.zeros_like(query))
            logits = lax.dot_general(
                masked, key, (((1,), (1,)), ((), ())), preferred_element_type=jnp.float32
            ) * factor
            logits = logits + (gates_t[i * tokens:keys, h:h + 1] - gates[h:h + 1, 0:keys])
            last = jnp.where(diagonal, logits[:, i * tokens:], -jnp.inf)
            logits = jnp.concatenate([logits[:, :i * tokens], last], axis=1) if i else last
            top = jnp.max(logits, axis=1, keepdims=True)
            scores = jnp.exp2(logits - top)
            total = jnp.sum(scores, axis=1, keepdims=True)
            weighted = jnp.dot(scores.astype(jnp.bfloat16), value, preferred_element_type=jnp.float32)
            result = jnp.where(lane == j, weighted / total, result)
        og[p, i * tokens:keys, :] = result.astype(jnp.bfloat16)

    out_copies = []

    def send_out(p):
        for d in order:
            peer = lax.rem(me + d, sp)
            copy = pltpu.make_async_remote_copy(
                src_ref=og.at[p, pl.ds(pl.multiple_of(peer * tokens, tokens), tokens), :],
                dst_ref=attended.at[:, pl.ds(pl.multiple_of(me * group + p * LANES, LANES), LANES)],
                send_sem=out_send.at[p, d - 1], recv_sem=out_recv.at[p, d - 1],
                device_id=(peer, mine), device_id_type=MESH)
            copy.start()
            out_copies.append(copy)
        copy = pltpu.make_async_copy(
            og.at[p, pl.ds(pl.multiple_of(me * tokens, tokens), tokens), :],
            attended.at[:, pl.ds(pl.multiple_of(me * group + p * LANES, LANES), LANES)],
            out_local.at[p])
        copy.start()
        own_copies.append(copy)

    done = 0
    for p in range(pairs):
        if done < steps:
            ring_step(done)
            done += 1
        for a in range(3):
            local_copies[p, a].wait()
            for d in order:
                qkv_copies[p, a, d].wait_recv()
        for i in range(sp):
            if i == sp // 2 and p == pairs - 1 and done < steps:
                ring_step(done)
                done += 1
            attend_block(p, i)
        send_out(p)
    while done < steps:
        ring_step(done)
        done += 1

    for copy in own_copies:
        copy.wait()
    for copy in out_copies:
        copy.wait()
    for copy in pair_copies.values():
        copy.wait()

    nt = (((1,), (1,)), ((), ()))
    for owner in range(dp):
        product = lax.dot_general(
            wg[owner], attended[...], nt, preferred_element_type=jnp.float32)
        out[owner * columns:(owner + 1) * columns, :] = product.astype(jnp.bfloat16)

    for copy in qkv_copies.values():
        copy.wait_send()
    for copy in ring_copies.values():
        copy.wait_send()


def fused(sp, dp, depth, q, k, v, gate, w):
    tokens, width = q.shape
    length = tokens * sp
    columns = w.shape[0]
    group = width // sp
    pairs = group // LANES
    steps = dp // 2
    any_spec = pl.BlockSpec(memory_space=pltpu.HBM)
    vmem_spec = pl.BlockSpec(memory_space=pltpu.VMEM)
    dma = pltpu.SemaphoreType.DMA
    gathered = pltpu.VMEM((pairs, length, LANES), jnp.bfloat16)
    return pl.pallas_call(
        functools.partial(fused_kernel, sp, dp, depth),
        out_shape=jax.ShapeDtypeStruct((columns * dp, tokens), jnp.bfloat16),
        in_specs=[any_spec, any_spec, any_spec, vmem_spec, any_spec],
        out_specs=vmem_spec,
        scratch_shapes=[
            gathered, gathered, gathered, gathered,
            pltpu.VMEM((tokens, width), jnp.bfloat16),
            pltpu.VMEM((dp, columns, width), jnp.bfloat16),
            dma((pairs, 3, sp - 1)), dma((pairs, 3, sp - 1)), dma((pairs, 3)),
            dma((pairs, sp - 1)), dma((pairs, sp - 1)), dma((pairs,)),
            dma((2, steps)), dma((2, steps)),
            dma((2, steps)), dma((2, steps)), dma((1,)),
        ],
        compiler_params=pltpu.CompilerParams(
            collective_id=0, has_side_effects=True, vmem_limit_bytes=48 * 1024 * 1024),
    )(q, k, v, gate, w)


def fits(sp, dp, tokens, width, depth, columns):
    return (
        sp % 2 == 0 and dp % 2 == 0 and dp >= 4
        and (width // sp) % LANES == 0 and LANES % depth == 0
        and tokens * sp <= 1024 and tokens % LANES == 0
        and width % (2 * LANES) == 0 and columns % 8 == 0
    )


def attend(query_all, key_all, value_all, gate_all):
    length, width = query_all.shape
    heads = gate_all.shape[0]
    depth = width // heads
    block_rows = min(512, length)
    block_count = length // block_rows
    score_scale = depth ** (-0.5)
    query_blocks = query_all.reshape(block_count, block_rows, heads, depth)
    key_blocks = key_all.reshape(block_count, block_rows, heads, depth)
    value_blocks = value_all.reshape(block_count, block_rows, heads, depth)
    gate_blocks = gate_all.reshape(heads, block_count, block_rows).transpose(1, 0, 2)
    offsets = jnp.arange(block_rows, dtype=jnp.int32)

    def one_block(block_index):
        query_part = lax.dynamic_index_in_dim(query_blocks, block_index, 0, keepdims=False)
        gate_part = lax.dynamic_index_in_dim(gate_blocks, block_index, 0, keepdims=False)
        query_rows = block_index * block_rows + offsets

        def key_step(key_block, carry):
            running_max, running_sum, weighted = carry
            key_part = lax.dynamic_index_in_dim(key_blocks, key_block, 0, keepdims=False)
            value_part = lax.dynamic_index_in_dim(value_blocks, key_block, 0, keepdims=False)
            gate_keys = lax.dynamic_index_in_dim(gate_blocks, key_block, 0, keepdims=False)
            logits = (
                jnp.einsum("qhe,khe->hqk", query_part, key_part, preferred_element_type=jnp.float32)
                * score_scale
            )
            logits = logits + gate_part[:, :, None] - gate_keys[:, None, :]
            key_rows = key_block * block_rows + offsets
            allowed = key_rows[None, :] <= query_rows[:, None]
            logits = jnp.where(allowed[None], logits, -jnp.inf)
            new_max = jnp.maximum(running_max, jnp.max(logits, axis=-1))
            scores = jnp.exp(logits - new_max[..., None])
            factor = jnp.exp(running_max - new_max)
            running_sum = running_sum * factor + jnp.sum(scores, axis=-1)
            weighted = weighted * factor[..., None] + jnp.einsum(
                "hqk,khe->hqe",
                scores.astype(jnp.bfloat16),
                value_part,
                preferred_element_type=jnp.float32,
            )
            return (new_max, running_sum, weighted)

        start_state = (
            jnp.full((heads, block_rows), -jnp.inf, jnp.float32),
            jnp.zeros((heads, block_rows), jnp.float32),
            jnp.zeros((heads, block_rows, depth), jnp.float32),
        )
        final_max, final_sum, weighted = lax.fori_loop(0, block_index + 1, key_step, start_state)
        result = weighted / final_sum[..., None]
        return result.transpose(1, 0, 2).astype(jnp.bfloat16)

    outputs = lax.map(one_block, jnp.arange(block_count, dtype=jnp.int32))
    return outputs.reshape(length, width)


def body(queries, keys, values, cum_gate, out_weight):
    sp, dp = lax.axis_size("sp"), lax.axis_size("dp")
    tokens, width = queries.shape[1:]
    depth = width // (cum_gate.shape[1] * sp)
    if fits(sp, dp, tokens, width, depth, out_weight.shape[1]):
        mixed = fused(sp, dp, depth, queries[0], keys[0], values[0], cum_gate[0], out_weight.T)
        return mixed.T[None]
    query_heads, key_heads, value_heads = (
        lax.all_to_all(queries, "sp", split_axis=2, concat_axis=1, tiled=True),
        lax.all_to_all(keys, "sp", split_axis=2, concat_axis=1, tiled=True),
        lax.all_to_all(values, "sp", split_axis=2, concat_axis=1, tiled=True),
    )
    local_out = attend(query_heads[0], key_heads[0], value_heads[0], cum_gate[0])
    attended = lax.all_to_all(local_out[None], "sp", split_axis=1, concat_axis=2, tiled=True)[0]
    group_rows = attended.shape[1] // lax.axis_size("sp")
    own_rows = lax.dynamic_slice_in_dim(
        out_weight, lax.axis_index("sp") * group_rows, group_rows, 0
    )
    full_rows = lax.all_gather(own_rows, "dp", axis=1, tiled=True)
    whole_weight = lax.all_gather(full_rows, "sp", axis=0, tiled=True)
    mixed = jnp.dot(attended, whole_weight, preferred_element_type=jnp.float32)
    return mixed.astype(jnp.bfloat16)[None]


def solution(mesh):
    in_specs = (
        P("dp", "sp", None),
        P("dp", "sp", None),
        P("dp", "sp", None),
        P("dp", "sp", None),
        P(None, "dp"),
    )
    out_specs = P("dp", "sp", None)
    return jax.shard_map(body, mesh=mesh, in_specs=in_specs, out_specs=out_specs, check_vma=False)
```

```python
import functools
import math

import jax
import jax.numpy as jnp
from jax import lax
from jax.experimental import pallas as pl
from jax.experimental.pallas import tpu as pltpu
from jax.sharding import PartitionSpec as P

LANES = 128
PACK = 8
PARTS = 3
CHUNKS = 2
ONES = 16
MESH = pl.DeviceIdType.MESH


def ring_index(position, n):
    upper = position // (n // 2)
    return (1 - upper) * (2 * position) + upper * (2 * (n - 1 - position) + 1)


def spans(total, pieces):
    units = total // PACK
    cuts = [PACK * (units * i // pieces) for i in range(pieces + 1)]
    return [(cuts[i], cuts[i + 1] - cuts[i]) for i in range(pieces)]


def fused_kernel(
    dp, depth, q, k, v, gate, w, out,
    qbuf, kbuf, vbuf, gown, gbuf, bias, vt, qx, ox, lx, oin, lin, oloc, lloc, att, wg, obuf,
    load_sem, kv_send, kv_recv, gate_send, gate_recv, qx_send, qx_recv,
    ox_send, ox_recv, lx_send, lx_recv, ring_send, ring_recv, pair_send, pair_recv, out_sem,
):
    tokens, width = q.shape
    columns = w.shape[0]
    pairs = width // LANES
    per_pair = LANES // depth
    own_heads = gown.shape[0]
    heads = width // depth
    both = 2 * tokens
    steps = dp // 2
    rounds = pairs // 2
    me = lax.axis_index("sp")
    mine = lax.axis_index("dp")
    core = lax.rem(me, 2)
    side_y = me // 2
    partner = me + 1 - 2 * core
    odd = lax.rem(mine, 2)
    position = (1 - odd) * (mine // 2) + odd * (dp - 1 - mine // 2)
    right = ring_index(lax.rem(position + 1, dp), dp)
    left = ring_index(lax.rem(position + dp - 1, dp), dp)
    low = side_y == 0
    high = side_y == 1

    def local(source, target, slot):
        copy = pltpu.make_async_copy(source, target, load_sem.at[slot])
        copy.start()
        return copy

    own_rows = pl.ds(pl.multiple_of(core * tokens, tokens), tokens)
    loads = [
        local(gate, gown, 0),
        local(k, kbuf.at[own_rows], 1),
        local(v, vbuf.at[own_rows], 2),
        local(q, qbuf, 3),
        local(w, wg.at[mine], 4),
    ]

    barrier = pltpu.get_barrier_semaphore()
    for d in range(1, 4):
        pl.semaphore_signal(
            barrier, inc=1, device_id=(lax.rem(me + d, 4), mine), device_id_type=MESH)
    for side in (left, right):
        pl.semaphore_signal(barrier, inc=1, device_id=(me, side), device_id_type=MESH)
    for copy in loads:
        copy.wait()
    gbuf[me] = gown[:, pl.ds(pl.multiple_of(side_y * both, both), both)]
    pl.semaphore_wait(barrier, 5)

    def remote(source, target, send, recv, device):
        return pltpu.make_async_remote_copy(
            src_ref=source, dst_ref=target, send_sem=send, recv_sem=recv,
            device_id=device, device_id_type=MESH)

    gate_copies = []
    for d in range(1, 4):
        peer = lax.rem(me + d, 4)
        gate_copies.append(remote(
            gown.at[:, pl.ds(pl.multiple_of((peer // 2) * both, both), both)],
            gbuf.at[me], gate_send.at[d - 1], gate_recv.at[d - 1], (peer, mine)))
    kv_copies = [
        remote(ref.at[own_rows], ref.at[own_rows], kv_send.at[i], kv_recv.at[i], (partner, mine))
        for i, ref in enumerate((kbuf, vbuf))
    ]

    def q_copy(p):
        return remote(
            qbuf.at[:, pl.ds(p * LANES, LANES)], qx.at[p, core],
            qx_send.at[p], qx_recv.at[p, core], (p % 2, mine))

    for copy in gate_copies:
        copy.start()
    for copy in kv_copies:
        copy.start()

    @pl.when(high)
    def _():
        for p in range(pairs):
            q_copy(p).start()

    half = width // 2
    lanes = pl.ds(pl.multiple_of(core * half, half), half)
    chunks = spans(columns, CHUNKS)
    events = steps * CHUNKS - CHUNKS // 2 if CHUNKS > 1 else steps
    ring_copies = {}
    pair_copies = {}

    def piece(owner, chunk):
        start, size = chunks[chunk]
        return wg.at[owner, pl.ds(start, size), lanes]

    def owner_of(side, step):
        shift = dp - 1 - step if side == 0 else 1 + step
        return ring_index(lax.rem(position + shift, dp), dp)

    def carries(side, step, chunk):
        if step < steps - 1:
            return True
        return (chunk < CHUNKS // 2) == (side == 0)

    def start_ring(side, step, chunk, owner):
        if not carries(side, step, chunk):
            return
        slot = step * CHUNKS + chunk
        copy = remote(
            piece(owner, chunk), piece(owner, chunk),
            ring_send.at[side, slot], ring_recv.at[side, slot],
            (me, right if side == 0 else left))
        copy.start()
        ring_copies[side, step, chunk] = copy

    def ring_event(step, index):
        for side in range(2):
            chunk = index
            if step == steps - 1:
                chunk = index + (CHUNKS // 2) * side
            owner = owner_of(side, step)
            ring_copies[side, step, chunk].wait_recv()
            if step + 1 < steps:
                start_ring(side, step + 1, chunk, owner)
            slot = step * CHUNKS + chunk
            copy = remote(
                piece(owner, chunk), piece(owner, chunk),
                pair_send.at[side, slot], pair_recv.at[side, slot], (partner, mine))
            copy.start()
            pair_copies[side, step, chunk] = copy

    for chunk in range(CHUNKS):
        for side in range(2):
            start_ring(side, 0, chunk, mine)

    scale = depth ** -0.5 * math.log2(math.e)
    for copy in kv_copies:
        copy.wait_recv()

    def transpose_values(p, carry):
        lane = pl.ds(pl.multiple_of(p * LANES, LANES), LANES)
        vt[p] = jnp.transpose(vbuf[:, lane])
        return carry

    lax.fori_loop(0, pairs, transpose_values, 0)

    for copy in gate_copies:
        copy.wait_recv()
    decay = jnp.concatenate([gbuf[i] for i in range(4)], axis=0) * (-(depth ** 0.5))
    rest = decay
    layers = []
    for _ in range(PARTS):
        layer = rest.astype(jnp.bfloat16).astype(jnp.float32)
        layers.append(layer)
        rest = rest - layer
    layers.append(jnp.zeros((LANES - PARTS * heads, both), jnp.float32))
    bias[...] = jnp.transpose(jnp.concatenate(layers, axis=0)).astype(jnp.bfloat16)

    bias_row = lax.broadcasted_iota(jnp.int32, (LANES, tokens), 0)
    ones = jnp.ones((ONES, both), jnp.bfloat16)

    def attend(p, query, keys, diagonal):
        lane = pl.ds(pl.multiple_of(p * LANES, LANES), LANES)
        turned = jnp.transpose(query)
        left_side = jnp.concatenate([kbuf[0:keys, lane], bias[0:keys, :]], axis=1)
        blank = jnp.zeros((depth, tokens), jnp.bfloat16)
        results = []
        for j in range(per_pair):
            head = p * per_pair + j
            picked = jnp.logical_and(
                lax.rem(bias_row, heads) == head, bias_row < PARTS * heads)
            parts = [blank] * per_pair
            parts[j] = turned[j * depth:(j + 1) * depth, :]
            right_side = jnp.concatenate(
                parts + [jnp.where(picked, 1.0, 0.0).astype(jnp.bfloat16)], axis=0)
            logits = jnp.dot(left_side, right_side, preferred_element_type=jnp.float32)
            if diagonal:
                first = keys - tokens
                allowed = (
                    lax.broadcasted_iota(jnp.int32, (tokens, tokens), 0)
                    <= lax.broadcasted_iota(jnp.int32, (tokens, tokens), 1))
                last = jnp.where(allowed, logits[first:, :], -jnp.inf)
                logits = jnp.concatenate([logits[:first, :], last], axis=0) if first else last
            top = jnp.max(logits, axis=0, keepdims=True)
            scores = jnp.exp2((logits - top) * scale).astype(jnp.bfloat16)
            weights = jnp.concatenate(
                [vt[p, j * depth:(j + 1) * depth, 0:keys], ones[:, 0:keys]], axis=0)
            summed = jnp.dot(weights, scores, preferred_element_type=jnp.float32)
            total = summed[depth:depth + 1, :]
            results.append((summed[:depth, :] * (1.0 / total), top * scale + jnp.log2(total)))
        return results

    def own_pair(p, keys):
        lane = pl.ds(pl.multiple_of(p * LANES, LANES), LANES)
        results = attend(p, qbuf[:, lane], keys, True)

        @pl.when(low)
        def _():
            for j in range(per_pair):
                att[p, j * depth:(j + 1) * depth, :] = results[j][0].astype(jnp.bfloat16)

        @pl.when(high)
        def _():
            for j in range(per_pair):
                oloc[p, j * depth:(j + 1) * depth, :] = results[j][0]
                lloc[p, j:j + 1, :] = results[j][1]

    def own_pairs(first, last):
        @pl.when(core == 0)
        def _():
            lax.fori_loop(first, last, lambda p, c: (own_pair(p, tokens), c)[1], 0)

        @pl.when(core == 1)
        def _():
            lax.fori_loop(first, last, lambda p, c: (own_pair(p, both), c)[1], 0)

    def o_copy(p, block):
        return remote(
            ox.at[p, block], oin.at[p], ox_send.at[p, block], ox_recv.at[p], (2 + block, mine))

    def l_copy(p, block):
        return remote(
            lx.at[p, block], lin.at[p], lx_send.at[p, block], lx_recv.at[p], (2 + block, mine))

    def other_pair(round_index):
        p = 2 * round_index + core

        def one(block, carry):
            remote(
                qbuf.at[:, pl.ds(0, LANES)], qx.at[p, block],
                qx_send.at[p], qx_recv.at[p, block], (partner, mine)).wait_recv()
            results = attend(p, qx[p, block], both, False)
            for j in range(per_pair):
                ox[p, block, j * depth:(j + 1) * depth, :] = results[j][0].astype(jnp.bfloat16)
                lx[p, block, j:j + 1, :] = results[j][1]
            o_copy(p, block).start()
            l_copy(p, block).start()
            return carry

        lax.fori_loop(0, 2, one, 0)

    def merge(p, carry):
        o_copy(p, 0).wait_recv()
        l_copy(p, 0).wait_recv()
        for j in range(per_pair):
            rows = pl.ds(j * depth, depth)
            near, far = lloc[p, j:j + 1, :], lin[p, j:j + 1, :]
            top = jnp.maximum(near, far)
            near, far = jnp.exp2(near - top), jnp.exp2(far - top)
            inverse = 1.0 / (near + far)
            mixed = oloc[p, rows, :] * (near * inverse) + oin[p, rows, :].astype(jnp.float32) * (far * inverse)
            att[p, rows, :] = mixed.astype(jnp.bfloat16)
        return carry

    out_copies = []

    def project(owner):
        slot = len(out_copies)
        total = jnp.dot(
            wg[owner], att[...].reshape(width, tokens), preferred_element_type=jnp.float32)
        obuf[slot] = total.astype(jnp.bfloat16)
        copy = pltpu.make_async_copy(
            obuf.at[slot], out.at[pl.ds(pl.multiple_of(owner * columns, PACK), columns)],
            out_sem.at[slot])
        copy.start()
        out_copies.append(copy)

    sequence = [(s, i) for s in range(steps - 1) for i in range(CHUNKS)]
    sequence += [(steps - 1, i) for i in range(max(CHUNKS // 2, 1))]
    merged = 0
    for r in range(rounds):
        own_pairs(r * pairs // rounds, (r + 1) * pairs // rounds)
        stop = min(max(2 * r - 1, 0), pairs)

        @pl.when(low)
        def _():
            other_pair(r)

        @pl.when(high)
        def _():
            lax.fori_loop(merged, stop, merge, 0)

        merged = stop
        ring_event(*sequence[r])

    @pl.when(high)
    def _():
        lax.fori_loop(merged, pairs, merge, 0)

    done = rounds
    ready = [(mine, -1)]
    projected = 0

    def arrived(step):
        for side in range(2):
            for chunk in range(CHUNKS):
                if (side, step, chunk) in pair_copies:
                    pair_copies[side, step, chunk].wait_recv()

    project(mine)
    for step in range(steps):
        while sum(1 for s, i in sequence[:done] if s == step) < sum(1 for s, i in sequence if s == step):
            ring_event(*sequence[done])
            done += 1
        arrived(step)
        if step < steps - 1:
            for side in range(2):
                project(owner_of(side, step))
        else:
            project(owner_of(0, step))

    for copy in out_copies:
        copy.wait()
    for copy in gate_copies + kv_copies + list(ring_copies.values()) + list(pair_copies.values()):
        copy.wait_send()

    @pl.when(high)
    def _():
        for p in range(pairs):
            q_copy(p).wait_send()

    @pl.when(low)
    def _():
        for r in range(rounds):
            for block in range(2):
                o_copy(2 * r + core, block).wait_send()
                l_copy(2 * r + core, block).wait_send()


def fused(dp, depth, q, k, v, gate, w):
    tokens, width = q.shape
    columns = w.shape[0]
    pairs = width // LANES
    both = 2 * tokens
    slots = dp // 2 * CHUNKS
    any_spec = pl.BlockSpec(memory_space=pl.ANY)
    dma = pltpu.SemaphoreType.DMA
    low, wide = jnp.bfloat16, jnp.float32
    per_pair = LANES // depth
    return pl.pallas_call(
        functools.partial(fused_kernel, dp, depth),
        out_shape=jax.ShapeDtypeStruct((columns * dp, tokens), low),
        in_specs=[any_spec] * 5,
        out_specs=any_spec,
        scratch_shapes=[
            pltpu.VMEM((tokens, width), low),
            pltpu.VMEM((both, width), low),
            pltpu.VMEM((both, width), low),
            pltpu.VMEM(gate.shape, wide),
            pltpu.VMEM((4, gate.shape[0], both), wide),
            pltpu.VMEM((both, LANES), low),
            pltpu.VMEM((pairs, LANES, both), low),
            pltpu.VMEM((pairs, 2, tokens, LANES), low),
            pltpu.VMEM((pairs, 2, LANES, tokens), low),
            pltpu.VMEM((pairs, 2, per_pair, tokens), wide),
            pltpu.VMEM((pairs, LANES, tokens), low),
            pltpu.VMEM((pairs, per_pair, tokens), wide),
            pltpu.VMEM((pairs, LANES, tokens), wide),
            pltpu.VMEM((pairs, per_pair, tokens), wide),
            pltpu.VMEM((pairs, LANES, tokens), low),
            pltpu.VMEM((dp, columns, width), low),
            pltpu.VMEM((dp, columns, tokens), low),
            dma((5,)), dma((2,)), dma((2,)), dma((3,)), dma((3,)),
            dma((pairs,)), dma((pairs, 2)),
            dma((pairs, 2)), dma((pairs,)), dma((pairs, 2)), dma((pairs,)),
            dma((2, slots)), dma((2, slots)), dma((2, slots)), dma((2, slots)),
            dma((dp,)),
        ],
        compiler_params=pltpu.CompilerParams(
            collective_id=0, has_side_effects=True, vmem_limit_bytes=63 * 1024 * 1024),
    )(q, k, v, gate, w)


def fits(sp, dp, tokens, width, depth, columns, own_heads):
    return (
        sp == 4 and dp % 2 == 0 and dp >= 4
        and tokens <= 256 and tokens % LANES == 0 and LANES % depth == 0 and depth % 16 == 0
        and width % (2 * LANES) == 0 and columns % PACK == 0 and columns >= 4 * PACK
        and own_heads * sp * depth == width and PARTS * own_heads * sp <= LANES
        and (width // LANES) % 2 == 0 and width // LANES // 2 <= (dp // 2) * CHUNKS - 1
    )


def attend(query_all, key_all, value_all, gate_all):
    length, width = query_all.shape
    heads = gate_all.shape[0]
    depth = width // heads
    block_rows = min(512, length)
    block_count = length // block_rows
    score_scale = depth ** (-0.5)
    query_blocks = query_all.reshape(block_count, block_rows, heads, depth)
    key_blocks = key_all.reshape(block_count, block_rows, heads, depth)
    value_blocks = value_all.reshape(block_count, block_rows, heads, depth)
    gate_blocks = gate_all.reshape(heads, block_count, block_rows).transpose(1, 0, 2)
    offsets = jnp.arange(block_rows, dtype=jnp.int32)

    def one_block(block_index):
        query_part = lax.dynamic_index_in_dim(query_blocks, block_index, 0, keepdims=False)
        gate_part = lax.dynamic_index_in_dim(gate_blocks, block_index, 0, keepdims=False)
        query_rows = block_index * block_rows + offsets

        def key_step(key_block, carry):
            running_max, running_sum, weighted = carry
            key_part = lax.dynamic_index_in_dim(key_blocks, key_block, 0, keepdims=False)
            value_part = lax.dynamic_index_in_dim(value_blocks, key_block, 0, keepdims=False)
            gate_keys = lax.dynamic_index_in_dim(gate_blocks, key_block, 0, keepdims=False)
            logits = (
                jnp.einsum("qhe,khe->hqk", query_part, key_part, preferred_element_type=jnp.float32)
                * score_scale
            )
            logits = logits + gate_part[:, :, None] - gate_keys[:, None, :]
            key_rows = key_block * block_rows + offsets
            allowed = key_rows[None, :] <= query_rows[:, None]
            logits = jnp.where(allowed[None], logits, -jnp.inf)
            new_max = jnp.maximum(running_max, jnp.max(logits, axis=-1))
            scores = jnp.exp(logits - new_max[..., None])
            factor = jnp.exp(running_max - new_max)
            running_sum = running_sum * factor + jnp.sum(scores, axis=-1)
            weighted = weighted * factor[..., None] + jnp.einsum(
                "hqk,khe->hqe",
                scores.astype(jnp.bfloat16),
                value_part,
                preferred_element_type=jnp.float32,
            )
            return (new_max, running_sum, weighted)

        start_state = (
            jnp.full((heads, block_rows), -jnp.inf, jnp.float32),
            jnp.zeros((heads, block_rows), jnp.float32),
            jnp.zeros((heads, block_rows, depth), jnp.float32),
        )
        final_max, final_sum, weighted = lax.fori_loop(0, block_index + 1, key_step, start_state)
        result = weighted / final_sum[..., None]
        return result.transpose(1, 0, 2).astype(jnp.bfloat16)

    outputs = lax.map(one_block, jnp.arange(block_count, dtype=jnp.int32))
    return outputs.reshape(length, width)


def body(queries, keys, values, cum_gate, out_weight):
    sp, dp = lax.axis_size("sp"), lax.axis_size("dp")
    tokens, width = queries.shape[1:]
    depth = width // (cum_gate.shape[1] * sp)
    if fits(sp, dp, tokens, width, depth, out_weight.shape[1], cum_gate.shape[1]):
        mixed = fused(dp, depth, queries[0], keys[0], values[0], cum_gate[0], out_weight.T)
        return mixed.T[None]
    query_heads, key_heads, value_heads = (
        lax.all_to_all(queries, "sp", split_axis=2, concat_axis=1, tiled=True),
        lax.all_to_all(keys, "sp", split_axis=2, concat_axis=1, tiled=True),
        lax.all_to_all(values, "sp", split_axis=2, concat_axis=1, tiled=True),
    )
    local_out = attend(query_heads[0], key_heads[0], value_heads[0], cum_gate[0])
    attended = lax.all_to_all(local_out[None], "sp", split_axis=1, concat_axis=2, tiled=True)[0]
    group_rows = attended.shape[1] // lax.axis_size("sp")
    own_rows = lax.dynamic_slice_in_dim(
        out_weight, lax.axis_index("sp") * group_rows, group_rows, 0
    )
    full_rows = lax.all_gather(own_rows, "dp", axis=1, tiled=True)
    whole_weight = lax.all_gather(full_rows, "sp", axis=0, tiled=True)
    mixed = jnp.dot(attended, whole_weight, preferred_element_type=jnp.float32)
    return mixed.astype(jnp.bfloat16)[None]


def solution(mesh):
    in_specs = (
        P("dp", "sp", None),
        P("dp", "sp", None),
        P("dp", "sp", None),
        P("dp", "sp", None),
        P(None, "dp"),
    )
    out_specs = P("dp", "sp", None)
    return jax.shard_map(body, mesh=mesh, in_specs=in_specs, out_specs=out_specs, check_vma=False)
```

```python
import functools
import math

import jax
import jax.numpy as jnp
from jax import lax
from jax.experimental import pallas as pl
from jax.experimental.pallas import tpu as pltpu
from jax.sharding import PartitionSpec as P

LANES = 128
PACK = 8
PARTS = 3
CHUNKS = 2
ONES = 16
MESH = pl.DeviceIdType.MESH


def ring_index(position, n):
    upper = position // (n // 2)
    return (1 - upper) * (2 * position) + upper * (2 * (n - 1 - position) + 1)


def spans(total, pieces):
    units = total // PACK
    cuts = [PACK * (units * i // pieces) for i in range(pieces + 1)]
    return [(cuts[i], cuts[i + 1] - cuts[i]) for i in range(pieces)]


def fused_kernel(
    dp, depth, q, k, v, gate, w, out,
    qbuf, kbuf, vbuf, gown, gbuf, bias, vt, qx, ox, lx, oin, lin, oloc, lloc, att, wg,
    load_sem, kv_send, kv_recv, gate_send, gate_recv, qx_send, qx_recv,
    ox_send, ox_recv, lx_send, lx_recv, ring_send, ring_recv, pair_send, pair_recv,
):
    tokens, width = q.shape
    columns = w.shape[0]
    pairs = width // LANES
    per_pair = LANES // depth
    own_heads = gown.shape[0]
    heads = width // depth
    both = 2 * tokens
    steps = dp // 2
    rounds = pairs // 2
    me = lax.axis_index("sp")
    mine = lax.axis_index("dp")
    core = lax.rem(me, 2)
    side_y = me // 2
    partner = me + 1 - 2 * core
    odd = lax.rem(mine, 2)
    position = (1 - odd) * (mine // 2) + odd * (dp - 1 - mine // 2)
    right = ring_index(lax.rem(position + 1, dp), dp)
    left = ring_index(lax.rem(position + dp - 1, dp), dp)
    low = side_y == 0
    high = side_y == 1

    def local(source, target, slot):
        copy = pltpu.make_async_copy(source, target, load_sem.at[slot])
        copy.start()
        return copy

    own_rows = pl.ds(pl.multiple_of(core * tokens, tokens), tokens)
    loads = [
        local(gate, gown, 0),
        local(k, kbuf.at[own_rows], 1),
        local(v, vbuf.at[own_rows], 2),
        local(q, qbuf, 3),
        local(w, wg.at[mine], 4),
    ]

    barrier = pltpu.get_barrier_semaphore()
    for d in range(1, 4):
        pl.semaphore_signal(
            barrier, inc=1, device_id=(lax.rem(me + d, 4), mine), device_id_type=MESH)
    for side in (left, right):
        pl.semaphore_signal(barrier, inc=1, device_id=(me, side), device_id_type=MESH)
    for copy in loads:
        copy.wait()
    gbuf[me] = gown[:, pl.ds(pl.multiple_of(side_y * both, both), both)]
    pl.semaphore_wait(barrier, 5)

    def remote(source, target, send, recv, device):
        return pltpu.make_async_remote_copy(
            src_ref=source, dst_ref=target, send_sem=send, recv_sem=recv,
            device_id=device, device_id_type=MESH)

    gate_copies = []
    for d in range(1, 4):
        peer = lax.rem(me + d, 4)
        gate_copies.append(remote(
            gown.at[:, pl.ds(pl.multiple_of((peer // 2) * both, both), both)],
            gbuf.at[me], gate_send.at[d - 1], gate_recv.at[d - 1], (peer, mine)))
    kv_copies = [
        remote(ref.at[own_rows], ref.at[own_rows], kv_send.at[i], kv_recv.at[i], (partner, mine))
        for i, ref in enumerate((kbuf, vbuf))
    ]

    def q_copy(p):
        return remote(
            qbuf.at[:, pl.ds(p * LANES, LANES)], qx.at[p, core],
            qx_send.at[p], qx_recv.at[p, core], (p % 2, mine))

    for copy in gate_copies:
        copy.start()
    for copy in kv_copies:
        copy.start()

    @pl.when(high)
    def _():
        for p in range(pairs):
            q_copy(p).start()

    half = width // 2
    lanes = pl.ds(pl.multiple_of(core * half, half), half)
    chunks = spans(columns, CHUNKS)
    events = steps * CHUNKS - CHUNKS // 2 if CHUNKS > 1 else steps
    ring_copies = {}
    pair_copies = {}

    def piece(owner, chunk):
        start, size = chunks[chunk]
        return wg.at[owner, pl.ds(start, size), lanes]

    def owner_of(side, step):
        shift = dp - 1 - step if side == 0 else 1 + step
        return ring_index(lax.rem(position + shift, dp), dp)

    def carries(side, step, chunk):
        if step < steps - 1:
            return True
        return (chunk < CHUNKS // 2) == (side == 0)

    def start_ring(side, step, chunk, owner):
        if not carries(side, step, chunk):
            return
        slot = step * CHUNKS + chunk
        copy = remote(
            piece(owner, chunk), piece(owner, chunk),
            ring_send.at[side, slot], ring_recv.at[side, slot],
            (me, right if side == 0 else left))
        copy.start()
        ring_copies[side, step, chunk] = copy

    def ring_event(step, index):
        for side in range(2):
            chunk = index
            if step == steps - 1:
                chunk = index + (CHUNKS // 2) * side
            owner = owner_of(side, step)
            ring_copies[side, step, chunk].wait_recv()
            if step + 1 < steps:
                start_ring(side, step + 1, chunk, owner)
            slot = step * CHUNKS + chunk
            copy = remote(
                piece(owner, chunk), piece(owner, chunk),
                pair_send.at[side, slot], pair_recv.at[side, slot], (partner, mine))
            copy.start()
            pair_copies[side, step, chunk] = copy

    for chunk in range(CHUNKS):
        for side in range(2):
            start_ring(side, 0, chunk, mine)

    scale = depth ** -0.5 * math.log2(math.e)
    for copy in kv_copies:
        copy.wait_recv()

    def transpose_values(p, carry):
        lane = pl.ds(pl.multiple_of(p * LANES, LANES), LANES)
        vt[p] = jnp.transpose(vbuf[:, lane])
        return carry

    lax.fori_loop(0, pairs, transpose_values, 0)

    for copy in gate_copies:
        copy.wait_recv()
    decay = jnp.concatenate([gbuf[i] for i in range(4)], axis=0) * (-(depth ** 0.5))
    rest = decay
    layers = []
    for _ in range(PARTS):
        layer = rest.astype(jnp.bfloat16).astype(jnp.float32)
        layers.append(layer)
        rest = rest - layer
    layers.append(jnp.zeros((LANES - PARTS * heads, both), jnp.float32))
    bias[...] = jnp.transpose(jnp.concatenate(layers, axis=0)).astype(jnp.bfloat16)

    bias_row = lax.broadcasted_iota(jnp.int32, (LANES, tokens), 0)
    ones = jnp.ones((ONES, both), jnp.bfloat16)

    def attend(p, query, keys, diagonal):
        lane = pl.ds(pl.multiple_of(p * LANES, LANES), LANES)
        turned = jnp.transpose(query)
        left_side = jnp.concatenate([kbuf[0:keys, lane], bias[0:keys, :]], axis=1)
        blank = jnp.zeros((depth, tokens), jnp.bfloat16)
        results = []
        for j in range(per_pair):
            head = p * per_pair + j
            picked = jnp.logical_and(
                lax.rem(bias_row, heads) == head, bias_row < PARTS * heads)
            parts = [blank] * per_pair
            parts[j] = turned[j * depth:(j + 1) * depth, :]
            right_side = jnp.concatenate(
                parts + [jnp.where(picked, 1.0, 0.0).astype(jnp.bfloat16)], axis=0)
            logits = jnp.dot(left_side, right_side, preferred_element_type=jnp.float32)
            if diagonal:
                first = keys - tokens
                allowed = (
                    lax.broadcasted_iota(jnp.int32, (tokens, tokens), 0)
                    <= lax.broadcasted_iota(jnp.int32, (tokens, tokens), 1))
                last = jnp.where(allowed, logits[first:, :], -jnp.inf)
                logits = jnp.concatenate([logits[:first, :], last], axis=0) if first else last
            top = jnp.max(logits, axis=0, keepdims=True)
            scores = jnp.exp2((logits - top) * scale).astype(jnp.bfloat16)
            weights = jnp.concatenate(
                [vt[p, j * depth:(j + 1) * depth, 0:keys], ones[:, 0:keys]], axis=0)
            summed = jnp.dot(weights, scores, preferred_element_type=jnp.float32)
            total = summed[depth:depth + 1, :]
            results.append((summed[:depth, :] * (1.0 / total), top * scale + jnp.log2(total)))
        return results

    def own_pair(p, keys):
        lane = pl.ds(pl.multiple_of(p * LANES, LANES), LANES)
        results = attend(p, qbuf[:, lane], keys, True)

        @pl.when(low)
        def _():
            for j in range(per_pair):
                att[p, j * depth:(j + 1) * depth, :] = results[j][0].astype(jnp.bfloat16)

        @pl.when(high)
        def _():
            for j in range(per_pair):
                oloc[p, j * depth:(j + 1) * depth, :] = results[j][0]
                lloc[p, j:j + 1, :] = results[j][1]

    def own_pairs(first, last):
        @pl.when(core == 0)
        def _():
            lax.fori_loop(first, last, lambda p, c: (own_pair(p, tokens), c)[1], 0)

        @pl.when(core == 1)
        def _():
            lax.fori_loop(first, last, lambda p, c: (own_pair(p, both), c)[1], 0)

    def o_copy(p, block):
        return remote(
            ox.at[p, block], oin.at[p], ox_send.at[p, block], ox_recv.at[p], (2 + block, mine))

    def l_copy(p, block):
        return remote(
            lx.at[p, block], lin.at[p], lx_send.at[p, block], lx_recv.at[p], (2 + block, mine))

    def other_pair(round_index):
        p = 2 * round_index + core

        def one(block, carry):
            remote(
                qbuf.at[:, pl.ds(0, LANES)], qx.at[p, block],
                qx_send.at[p], qx_recv.at[p, block], (partner, mine)).wait_recv()
            results = attend(p, qx[p, block], both, False)
            for j in range(per_pair):
                ox[p, block, j * depth:(j + 1) * depth, :] = results[j][0].astype(jnp.bfloat16)
                lx[p, block, j:j + 1, :] = results[j][1]
            o_copy(p, block).start()
            l_copy(p, block).start()
            return carry

        lax.fori_loop(0, 2, one, 0)

    def merge(p, carry):
        o_copy(p, 0).wait_recv()
        l_copy(p, 0).wait_recv()
        for j in range(per_pair):
            rows = pl.ds(j * depth, depth)
            near, far = lloc[p, j:j + 1, :], lin[p, j:j + 1, :]
            top = jnp.maximum(near, far)
            near, far = jnp.exp2(near - top), jnp.exp2(far - top)
            inverse = 1.0 / (near + far)
            mixed = oloc[p, rows, :] * (near * inverse) + oin[p, rows, :].astype(jnp.float32) * (far * inverse)
            att[p, rows, :] = mixed.astype(jnp.bfloat16)
        return carry

    def project(owner):
        total = jnp.dot(
            wg[owner], att[...].reshape(width, tokens), preferred_element_type=jnp.float32)
        out[pl.ds(pl.multiple_of(owner * columns, PACK), columns), :] = total.astype(jnp.bfloat16)

    sequence = [(s, i) for s in range(steps - 1) for i in range(CHUNKS)]
    sequence += [(steps - 1, i) for i in range(max(CHUNKS // 2, 1))]
    merged = 0
    for r in range(rounds):
        own_pairs(r * pairs // rounds, (r + 1) * pairs // rounds)
        stop = min(max(2 * r - 1, 0), pairs)

        @pl.when(low)
        def _():
            other_pair(r)

        @pl.when(high)
        def _():
            lax.fori_loop(merged, stop, merge, 0)

        merged = stop
        ring_event(*sequence[r])

    @pl.when(high)
    def _():
        lax.fori_loop(merged, pairs, merge, 0)

    done = rounds
    ready = [(mine, -1)]
    projected = 0

    def arrived(step):
        for side in range(2):
            for chunk in range(CHUNKS):
                if (side, step, chunk) in pair_copies:
                    pair_copies[side, step, chunk].wait_recv()

    project(mine)
    for step in range(steps):
        while sum(1 for s, i in sequence[:done] if s == step) < sum(1 for s, i in sequence if s == step):
            ring_event(*sequence[done])
            done += 1
        arrived(step)
        if step < steps - 1:
            for side in range(2):
                project(owner_of(side, step))
        else:
            project(owner_of(0, step))

    for copy in gate_copies + kv_copies + list(ring_copies.values()) + list(pair_copies.values()):
        copy.wait_send()

    @pl.when(high)
    def _():
        for p in range(pairs):
            q_copy(p).wait_send()

    @pl.when(low)
    def _():
        for r in range(rounds):
            for block in range(2):
                o_copy(2 * r + core, block).wait_send()
                l_copy(2 * r + core, block).wait_send()


def fused(dp, depth, q, k, v, gate, w):
    tokens, width = q.shape
    columns = w.shape[0]
    pairs = width // LANES
    both = 2 * tokens
    slots = dp // 2 * CHUNKS
    any_spec = pl.BlockSpec(memory_space=pl.ANY)
    dma = pltpu.SemaphoreType.DMA
    low, wide = jnp.bfloat16, jnp.float32
    per_pair = LANES // depth
    return pl.pallas_call(
        functools.partial(fused_kernel, dp, depth),
        out_shape=pltpu.VMEM((columns * dp, tokens), low),
        in_specs=[any_spec] * 5,
        out_specs=pl.BlockSpec(memory_space=pltpu.VMEM),
        scratch_shapes=[
            pltpu.VMEM((tokens, width), low),
            pltpu.VMEM((both, width), low),
            pltpu.VMEM((both, width), low),
            pltpu.VMEM(gate.shape, wide),
            pltpu.VMEM((4, gate.shape[0], both), wide),
            pltpu.VMEM((both, LANES), low),
            pltpu.VMEM((pairs, LANES, both), low),
            pltpu.VMEM((pairs, 2, tokens, LANES), low),
            pltpu.VMEM((pairs, 2, LANES, tokens), low),
            pltpu.VMEM((pairs, 2, per_pair, tokens), wide),
            pltpu.VMEM((pairs, LANES, tokens), low),
            pltpu.VMEM((pairs, per_pair, tokens), wide),
            pltpu.VMEM((pairs, LANES, tokens), wide),
            pltpu.VMEM((pairs, per_pair, tokens), wide),
            pltpu.VMEM((pairs, LANES, tokens), low),
            pltpu.VMEM((dp, columns, width), low),
            dma((5,)), dma((2,)), dma((2,)), dma((3,)), dma((3,)),
            dma((pairs,)), dma((pairs, 2)),
            dma((pairs, 2)), dma((pairs,)), dma((pairs, 2)), dma((pairs,)),
            dma((2, slots)), dma((2, slots)), dma((2, slots)), dma((2, slots)),
        ],
        compiler_params=pltpu.CompilerParams(
            collective_id=0, has_side_effects=True, vmem_limit_bytes=48 * 1024 * 1024),
    )(*(pltpu.with_memory_space_constraint(x, pltpu.HBM) for x in (q, k, v, gate, w)))


def fits(sp, dp, tokens, width, depth, columns, own_heads):
    return (
        sp == 4 and dp % 2 == 0 and dp >= 4
        and tokens <= 256 and tokens % LANES == 0 and LANES % depth == 0 and depth % 16 == 0
        and width % (2 * LANES) == 0 and columns % PACK == 0 and columns >= 4 * PACK
        and own_heads * sp * depth == width and PARTS * own_heads * sp <= LANES
        and (width // LANES) % 2 == 0 and width // LANES // 2 <= (dp // 2) * CHUNKS - 1
    )


def attend(query_all, key_all, value_all, gate_all):
    length, width = query_all.shape
    heads = gate_all.shape[0]
    depth = width // heads
    block_rows = min(512, length)
    block_count = length // block_rows
    score_scale = depth ** (-0.5)
    query_blocks = query_all.reshape(block_count, block_rows, heads, depth)
    key_blocks = key_all.reshape(block_count, block_rows, heads, depth)
    value_blocks = value_all.reshape(block_count, block_rows, heads, depth)
    gate_blocks = gate_all.reshape(heads, block_count, block_rows).transpose(1, 0, 2)
    offsets = jnp.arange(block_rows, dtype=jnp.int32)

    def one_block(block_index):
        query_part = lax.dynamic_index_in_dim(query_blocks, block_index, 0, keepdims=False)
        gate_part = lax.dynamic_index_in_dim(gate_blocks, block_index, 0, keepdims=False)
        query_rows = block_index * block_rows + offsets

        def key_step(key_block, carry):
            running_max, running_sum, weighted = carry
            key_part = lax.dynamic_index_in_dim(key_blocks, key_block, 0, keepdims=False)
            value_part = lax.dynamic_index_in_dim(value_blocks, key_block, 0, keepdims=False)
            gate_keys = lax.dynamic_index_in_dim(gate_blocks, key_block, 0, keepdims=False)
            logits = (
                jnp.einsum("qhe,khe->hqk", query_part, key_part, preferred_element_type=jnp.float32)
                * score_scale
            )
            logits = logits + gate_part[:, :, None] - gate_keys[:, None, :]
            key_rows = key_block * block_rows + offsets
            allowed = key_rows[None, :] <= query_rows[:, None]
            logits = jnp.where(allowed[None], logits, -jnp.inf)
            new_max = jnp.maximum(running_max, jnp.max(logits, axis=-1))
            scores = jnp.exp(logits - new_max[..., None])
            factor = jnp.exp(running_max - new_max)
            running_sum = running_sum * factor + jnp.sum(scores, axis=-1)
            weighted = weighted * factor[..., None] + jnp.einsum(
                "hqk,khe->hqe",
                scores.astype(jnp.bfloat16),
                value_part,
                preferred_element_type=jnp.float32,
            )
            return (new_max, running_sum, weighted)

        start_state = (
            jnp.full((heads, block_rows), -jnp.inf, jnp.float32),
            jnp.zeros((heads, block_rows), jnp.float32),
            jnp.zeros((heads, block_rows, depth), jnp.float32),
        )
        final_max, final_sum, weighted = lax.fori_loop(0, block_index + 1, key_step, start_state)
        result = weighted / final_sum[..., None]
        return result.transpose(1, 0, 2).astype(jnp.bfloat16)

    outputs = lax.map(one_block, jnp.arange(block_count, dtype=jnp.int32))
    return outputs.reshape(length, width)


def body(queries, keys, values, cum_gate, out_weight):
    sp, dp = lax.axis_size("sp"), lax.axis_size("dp")
    tokens, width = queries.shape[1:]
    depth = width // (cum_gate.shape[1] * sp)
    if fits(sp, dp, tokens, width, depth, out_weight.shape[1], cum_gate.shape[1]):
        mixed = fused(dp, depth, queries[0], keys[0], values[0], cum_gate[0], out_weight.T)
        return mixed.T[None]
    query_heads, key_heads, value_heads = (
        lax.all_to_all(queries, "sp", split_axis=2, concat_axis=1, tiled=True),
        lax.all_to_all(keys, "sp", split_axis=2, concat_axis=1, tiled=True),
        lax.all_to_all(values, "sp", split_axis=2, concat_axis=1, tiled=True),
    )
    local_out = attend(query_heads[0], key_heads[0], value_heads[0], cum_gate[0])
    attended = lax.all_to_all(local_out[None], "sp", split_axis=1, concat_axis=2, tiled=True)[0]
    group_rows = attended.shape[1] // lax.axis_size("sp")
    own_rows = lax.dynamic_slice_in_dim(
        out_weight, lax.axis_index("sp") * group_rows, group_rows, 0
    )
    full_rows = lax.all_gather(own_rows, "dp", axis=1, tiled=True)
    whole_weight = lax.all_gather(full_rows, "sp", axis=0, tiled=True)
    mixed = jnp.dot(attended, whole_weight, preferred_element_type=jnp.float32)
    return mixed.astype(jnp.bfloat16)[None]


def solution(mesh):
    in_specs = (
        P("dp", "sp", None),
        P("dp", "sp", None),
        P("dp", "sp", None),
        P("dp", "sp", None),
        P(None, "dp"),
    )
    out_specs = P("dp", "sp", None)
    return jax.shard_map(body, mesh=mesh, in_specs=in_specs, out_specs=out_specs, check_vma=False)
```

```python
import functools
import math

import jax
import jax.numpy as jnp
from jax import lax
from jax.experimental import pallas as pl
from jax.experimental.pallas import tpu as pltpu
from jax.sharding import PartitionSpec as P

LANES = 128
PACK = 8
PARTS = 3
ONES = 16
MESH = pl.DeviceIdType.MESH


def ring_index(position, n):
    upper = position // (n // 2)
    return (1 - upper) * (2 * position) + upper * (2 * (n - 1 - position) + 1)


def pieces_of(columns):
    units = columns // PACK
    half = -(-units // 2)
    sizes = [-(-half // 2), half // 2, -(-(units - half) // 2), (units - half) // 2]
    starts = [sum(sizes[:i]) for i in range(4)]
    return [(PACK * start, PACK * size) for start, size in zip(starts, sizes)]


def fused_kernel(
    dp, depth, q, k, v, gate, w, out,
    qbuf, kbuf, vbuf, gown, gbuf, bias, qt, vt, qx, ox, lx, oin, lin, oloc, lloc, att, wg,
    load_sem, kv_send, kv_recv, gate_send, gate_recv, qx_send, qx_recv,
    ox_send, ox_recv, lx_send, lx_recv, ring_send, ring_recv, pair_send, pair_recv,
):
    tokens, width = q.shape
    columns = w.shape[0]
    pairs = width // LANES
    per_pair = LANES // depth
    own_heads = gown.shape[0]
    heads = width // depth
    both = 2 * tokens
    steps = dp // 2
    rounds = pairs // 2
    me = lax.axis_index("sp")
    mine = lax.axis_index("dp")
    core = lax.rem(me, 2)
    side_y = me // 2
    partner = me + 1 - 2 * core
    odd = lax.rem(mine, 2)
    position = (1 - odd) * (mine // 2) + odd * (dp - 1 - mine // 2)
    right = ring_index(lax.rem(position + 1, dp), dp)
    left = ring_index(lax.rem(position + dp - 1, dp), dp)
    low = side_y == 0
    high = side_y == 1

    def local(source, target, slot):
        copy = pltpu.make_async_copy(source, target, load_sem.at[slot])
        copy.start()
        return copy

    own_rows = pl.ds(pl.multiple_of(core * tokens, tokens), tokens)
    loads = [
        local(gate, gown, 0),
        local(k, kbuf.at[own_rows], 1),
        local(v, vbuf.at[own_rows], 2),
        local(q, qbuf, 3),
        local(w, wg.at[mine], 4),
    ]

    barrier = pltpu.get_barrier_semaphore()
    for d in range(1, 4):
        pl.semaphore_signal(
            barrier, inc=1, device_id=(lax.rem(me + d, 4), mine), device_id_type=MESH)

    @pl.when(core == 1)
    def _():
        for side in (left, right):
            pl.semaphore_signal(barrier, inc=1, device_id=(me, side), device_id_type=MESH)

    for copy in loads:
        copy.wait()
    gbuf[me] = gown[:, pl.ds(pl.multiple_of(side_y * both, both), both)]

    def turn(start, with_queries):
        columns_here = pl.ds(pl.multiple_of(start, tokens), tokens)

        def one(p, carry):
            lane = pl.ds(pl.multiple_of(p * LANES, LANES), LANES)
            if with_queries:
                qt[p] = jnp.transpose(qbuf[:, lane])
            vt[p, :, columns_here] = jnp.transpose(vbuf[columns_here, lane])
            return carry

        lax.fori_loop(0, pairs, one, 0)

    turn(core * tokens, True)

    @pl.when(core == 0)
    def _():
        pl.semaphore_wait(barrier, 3)

    @pl.when(core == 1)
    def _():
        pl.semaphore_wait(barrier, 5)


    def remote(source, target, send, recv, device):
        return pltpu.make_async_remote_copy(
            src_ref=source, dst_ref=target, send_sem=send, recv_sem=recv,
            device_id=device, device_id_type=MESH)

    gate_copies = []
    for d in range(1, 4):
        peer = lax.rem(me + d, 4)
        gate_copies.append(remote(
            gown.at[:, pl.ds(pl.multiple_of((peer // 2) * both, both), both)],
            gbuf.at[me], gate_send.at[d - 1], gate_recv.at[d - 1], (peer, mine)))
    kv_copies = [
        remote(ref.at[own_rows], ref.at[own_rows], kv_send.at[i], kv_recv.at[i], (partner, mine))
        for i, ref in enumerate((kbuf, vbuf))
    ]

    def q_copy(p):
        return remote(
            qbuf.at[:, pl.ds(p * LANES, LANES)], qx.at[p, core],
            qx_send.at[p], qx_recv.at[p, core], (0, mine))

    for copy in gate_copies:
        copy.start()
    for copy in kv_copies:
        copy.start()

    parts = pieces_of(columns)

    def piece(owner, part):
        start, size = parts[part]
        return wg.at[owner, pl.ds(start, size)]

    def owner_of(side, step):
        shift = dp - 1 - step if side == 0 else 1 + step
        return ring_index(lax.rem(position + shift, dp), dp)

    def carries(side, step, part):
        return step < steps - 1 or (part < 2) == (side == 0)

    def ring_copy(side, step, part):
        here = piece(owner_of(side, step - 1) if step else mine, part)
        slot = step * 4 + part
        return remote(
            here, here, ring_send.at[side, slot], ring_recv.at[side, slot],
            (me, right if side == 0 else left))

    def pair_copy(side, step, part):
        here = piece(owner_of(side, step), part)
        slot = step * 4 + part
        return remote(
            here, here, pair_send.at[side, slot], pair_recv.at[side, slot], (partner, mine))

    def sides_of(step):
        return range(2 if step < steps - 1 else 1)

    def ring_event(side, step, part):
        ring_copy(side, step, part).wait_recv()
        if step + 1 < steps and carries(side, step + 1, part):
            ring_copy(side, step + 1, part).start()
        pair_copy(side, step, part).start()

    every = [
        (side, step, part) for step in range(steps) for part in range(4) for side in range(2)
        if carries(side, step, part)]

    @pl.when(core == 1)
    def _():
        for part in range(4):
            for side in range(2):
                ring_copy(side, 0, part).start()

    @pl.when(high)
    def _():
        for p in range(pairs):
            q_copy(p).start()

    scale = depth ** -0.5 * math.log2(math.e)
    for copy in kv_copies:
        copy.wait_recv()

    turn((1 - core) * tokens, False)
    for copy in gate_copies:
        copy.wait_recv()
    decay = jnp.concatenate([gbuf[i] for i in range(4)], axis=0) * (-(depth ** 0.5))
    rest = decay
    layers = []
    for _ in range(PARTS):
        layer = rest.astype(jnp.bfloat16).astype(jnp.float32)
        layers.append(layer)
        rest = rest - layer
    layers.append(jnp.zeros((LANES - PARTS * heads, both), jnp.float32))
    bias[...] = jnp.transpose(jnp.concatenate(layers, axis=0)).astype(jnp.bfloat16)

    bias_row = lax.broadcasted_iota(jnp.int32, (LANES, tokens), 0)
    ones = jnp.ones((ONES, both), jnp.bfloat16)

    def attend(items, keys, diagonal):
        blank = jnp.zeros((depth, tokens), jnp.bfloat16)
        logits = []
        for p, turned in items:
            lane = pl.ds(pl.multiple_of(p * LANES, LANES), LANES)
            left_side = jnp.concatenate([kbuf[0:keys, lane], bias[0:keys, :]], axis=1)
            for j in range(per_pair):
                head = p * per_pair + j
                picked = jnp.logical_and(
                    lax.rem(bias_row, heads) == head, bias_row < PARTS * heads)
                rows = [blank] * per_pair
                rows[j] = turned[j * depth:(j + 1) * depth, :]
                right_side = jnp.concatenate(
                    rows + [jnp.where(picked, 1.0, 0.0).astype(jnp.bfloat16)], axis=0)
                logits.append(
                    jnp.dot(left_side, right_side, preferred_element_type=jnp.float32))
        if diagonal:
            first = keys - tokens
            allowed = (
                lax.broadcasted_iota(jnp.int32, (tokens, tokens), 0)
                <= lax.broadcasted_iota(jnp.int32, (tokens, tokens), 1))
            for n, plain in enumerate(logits):
                last = jnp.where(allowed, plain[first:, :], -jnp.inf)
                logits[n] = jnp.concatenate([plain[:first, :], last], axis=0) if first else last
        tops = [jnp.max(x, axis=0, keepdims=True) for x in logits]
        scores = [
            jnp.exp2((x - top) * scale).astype(jnp.bfloat16) for x, top in zip(logits, tops)]
        results = []
        for i, (p, _) in enumerate(items):
            found = []
            for j in range(per_pair):
                n = i * per_pair + j
                weights = jnp.concatenate(
                    [vt[p, j * depth:(j + 1) * depth, 0:keys], ones[:, 0:keys]], axis=0)
                summed = jnp.dot(weights, scores[n], preferred_element_type=jnp.float32)
                total = summed[depth:depth + 1, :]
                found.append(
                    (summed[:depth, :] * (1.0 / total), tops[n] * scale + jnp.log2(total)))
            results.append(found)
        return results

    def own_pairs(first, last, keys):
        span = range(first, last)
        results = attend([(p, qt[p]) for p in span], keys, True)

        @pl.when(low)
        def _():
            for p, found in zip(span, results):
                for j in range(per_pair):
                    att[p, j * depth:(j + 1) * depth, :] = found[j][0].astype(jnp.bfloat16)

        @pl.when(high)
        def _():
            for p, found in zip(span, results):
                for j in range(per_pair):
                    oloc[p, j * depth:(j + 1) * depth, :] = found[j][0]
                    lloc[p, j:j + 1, :] = found[j][1]

    def o_copy(p, block):
        return remote(
            ox.at[p, block], oin.at[p], ox_send.at[p, block], ox_recv.at[p], (2 + block, mine))

    def l_copy(p, block):
        return remote(
            lx.at[p, block], lin.at[p], lx_send.at[p, block], lx_recv.at[p], (2 + block, mine))

    def other_pair(p):
        for block in range(2):
            remote(
                qbuf.at[:, pl.ds(0, LANES)], qx.at[p, block],
                qx_send.at[p], qx_recv.at[p, block], (partner, mine)).wait_recv()
        results = attend([(p, jnp.transpose(qx[p, block])) for block in range(2)], both, False)
        for block in range(2):
            for j in range(per_pair):
                found = results[block][j]
                ox[p, block, j * depth:(j + 1) * depth, :] = found[0].astype(jnp.bfloat16)
                lx[p, block, j:j + 1, :] = found[1]
            o_copy(p, block).start()
            l_copy(p, block).start()

    def merge(p, carry):
        o_copy(p, 0).wait_recv()
        l_copy(p, 0).wait_recv()
        for j in range(per_pair):
            rows = pl.ds(j * depth, depth)
            near, far = lloc[p, j:j + 1, :], lin[p, j:j + 1, :]
            top = jnp.maximum(near, far)
            near, far = jnp.exp2(near - top), jnp.exp2(far - top)
            inverse = 1.0 / (near + far)
            mixed = oloc[p, rows, :] * (near * inverse) + oin[p, rows, :].astype(jnp.float32) * (far * inverse)
            att[p, rows, :] = mixed.astype(jnp.bfloat16)
        return carry

    def project(owner):
        total = jnp.dot(
            wg[owner], att[...].reshape(width, tokens), preferred_element_type=jnp.float32)
        out[pl.ds(pl.multiple_of(owner * columns, PACK), columns), :] = total.astype(jnp.bfloat16)

    def merge_to(first, last):
        @pl.when(high)
        def _():
            lax.fori_loop(first, last, merge, 0)

    def finish(step):
        for side in sides_of(step):
            project(owner_of(side, step))

    @pl.when(core == 0)
    def _():
        for r in range(rounds):
            own_pairs(r * pairs // rounds, (r + 1) * pairs // rounds, tokens)

        @pl.when(low)
        def _():
            for p in range(pairs):
                other_pair(p)

        merge_to(0, pairs)
        project(mine)
        for step in range(steps):
            for key in every:
                if key[1] == step:
                    pair_copy(*key).wait_recv()
            finish(step)

        @pl.when(low)
        def _():
            for p in range(pairs):
                for block in range(2):
                    o_copy(p, block).wait_send()
                    l_copy(p, block).wait_send()

    @pl.when(core == 1)
    def _():
        todo = list(every)

        def advance(count):
            for _ in range(count):
                ring_event(*todo.pop(0))

        for r in range(rounds):
            own_pairs(r * pairs // rounds, (r + 1) * pairs // rounds, both)
            advance(2)
        while todo and todo[0][1] < steps - 1:
            advance(1)
        merge_to(0, pairs)
        project(mine)
        for step in range(steps - 1):
            finish(step)
        advance(len(todo))
        finish(steps - 1)
        for key in every:
            ring_copy(*key).wait_send()
            pair_copy(*key).wait_send()

    for copy in gate_copies + kv_copies:
        copy.wait_send()

    @pl.when(high)
    def _():
        for p in range(pairs):
            q_copy(p).wait_send()


def fused(dp, depth, q, k, v, gate, w):
    tokens, width = q.shape
    columns = w.shape[0]
    pairs = width // LANES
    both = 2 * tokens
    steps = dp // 2
    slots = steps * 4
    any_spec = pl.BlockSpec(memory_space=pl.ANY)
    dma = pltpu.SemaphoreType.DMA
    low, wide = jnp.bfloat16, jnp.float32
    per_pair = LANES // depth
    return pl.pallas_call(
        functools.partial(fused_kernel, dp, depth),
        out_shape=pltpu.VMEM((columns * dp, tokens), low),
        in_specs=[any_spec] * 5,
        out_specs=pl.BlockSpec(memory_space=pltpu.VMEM),
        scratch_shapes=[
            pltpu.VMEM((tokens, width), low),
            pltpu.VMEM((both, width), low),
            pltpu.VMEM((both, width), low),
            pltpu.VMEM(gate.shape, wide),
            pltpu.VMEM((4, gate.shape[0], both), wide),
            pltpu.VMEM((both, LANES), low),
            pltpu.VMEM((pairs, LANES, tokens), low),
            pltpu.VMEM((pairs, LANES, both), low),
            pltpu.VMEM((pairs, 2, tokens, LANES), low),
            pltpu.VMEM((pairs, 2, LANES, tokens), low),
            pltpu.VMEM((pairs, 2, per_pair, tokens), wide),
            pltpu.VMEM((pairs, LANES, tokens), low),
            pltpu.VMEM((pairs, per_pair, tokens), wide),
            pltpu.VMEM((pairs, LANES, tokens), wide),
            pltpu.VMEM((pairs, per_pair, tokens), wide),
            pltpu.VMEM((pairs, LANES, tokens), low),
            pltpu.VMEM((dp, columns, width), low),
            dma((5,)), dma((2,)), dma((2,)), dma((3,)), dma((3,)),
            dma((pairs,)), dma((pairs, 2)),
            dma((pairs, 2)), dma((pairs,)), dma((pairs, 2)), dma((pairs,)),
            dma((2, slots)), dma((2, slots)), dma((2, slots)), dma((2, slots)),
        ],
        compiler_params=pltpu.CompilerParams(
            collective_id=0, has_side_effects=True, vmem_limit_bytes=48 * 1024 * 1024),
    )(*(pltpu.with_memory_space_constraint(x, pltpu.HBM) for x in (q, k, v, gate, w)))


def fits(sp, dp, tokens, width, depth, columns, own_heads):
    return (
        sp == 4 and dp % 2 == 0 and dp >= 4
        and tokens <= 256 and tokens % LANES == 0 and LANES % depth == 0 and depth % 16 == 0
        and width % (2 * LANES) == 0 and columns % PACK == 0 and columns >= 4 * PACK
        and own_heads * sp * depth == width and PARTS * own_heads * sp <= LANES
        and width == 8 * LANES and dp == 8
    )


def attend(query_all, key_all, value_all, gate_all):
    length, width = query_all.shape
    heads = gate_all.shape[0]
    depth = width // heads
    block_rows = min(512, length)
    block_count = length // block_rows
    score_scale = depth ** (-0.5)
    query_blocks = query_all.reshape(block_count, block_rows, heads, depth)
    key_blocks = key_all.reshape(block_count, block_rows, heads, depth)
    value_blocks = value_all.reshape(block_count, block_rows, heads, depth)
    gate_blocks = gate_all.reshape(heads, block_count, block_rows).transpose(1, 0, 2)
    offsets = jnp.arange(block_rows, dtype=jnp.int32)

    def one_block(block_index):
        query_part = lax.dynamic_index_in_dim(query_blocks, block_index, 0, keepdims=False)
        gate_part = lax.dynamic_index_in_dim(gate_blocks, block_index, 0, keepdims=False)
        query_rows = block_index * block_rows + offsets

        def key_step(key_block, carry):
            running_max, running_sum, weighted = carry
            key_part = lax.dynamic_index_in_dim(key_blocks, key_block, 0, keepdims=False)
            value_part = lax.dynamic_index_in_dim(value_blocks, key_block, 0, keepdims=False)
            gate_keys = lax.dynamic_index_in_dim(gate_blocks, key_block, 0, keepdims=False)
            logits = (
                jnp.einsum("qhe,khe->hqk", query_part, key_part, preferred_element_type=jnp.float32)
                * score_scale
            )
            logits = logits + gate_part[:, :, None] - gate_keys[:, None, :]
            key_rows = key_block * block_rows + offsets
            allowed = key_rows[None, :] <= query_rows[:, None]
            logits = jnp.where(allowed[None], logits, -jnp.inf)
            new_max = jnp.maximum(running_max, jnp.max(logits, axis=-1))
            scores = jnp.exp(logits - new_max[..., None])
            factor = jnp.exp(running_max - new_max)
            running_sum = running_sum * factor + jnp.sum(scores, axis=-1)
            weighted = weighted * factor[..., None] + jnp.einsum(
                "hqk,khe->hqe",
                scores.astype(jnp.bfloat16),
                value_part,
                preferred_element_type=jnp.float32,
            )
            return (new_max, running_sum, weighted)

        start_state = (
            jnp.full((heads, block_rows), -jnp.inf, jnp.float32),
            jnp.zeros((heads, block_rows), jnp.float32),
            jnp.zeros((heads, block_rows, depth), jnp.float32),
        )
        final_max, final_sum, weighted = lax.fori_loop(0, block_index + 1, key_step, start_state)
        result = weighted / final_sum[..., None]
        return result.transpose(1, 0, 2).astype(jnp.bfloat16)

    outputs = lax.map(one_block, jnp.arange(block_count, dtype=jnp.int32))
    return outputs.reshape(length, width)


def body(queries, keys, values, cum_gate, out_weight):
    sp, dp = lax.axis_size("sp"), lax.axis_size("dp")
    tokens, width = queries.shape[1:]
    depth = width // (cum_gate.shape[1] * sp)
    if fits(sp, dp, tokens, width, depth, out_weight.shape[1], cum_gate.shape[1]):
        mixed = fused(dp, depth, queries[0], keys[0], values[0], cum_gate[0], out_weight.T)
        return mixed.T[None]
    query_heads, key_heads, value_heads = (
        lax.all_to_all(queries, "sp", split_axis=2, concat_axis=1, tiled=True),
        lax.all_to_all(keys, "sp", split_axis=2, concat_axis=1, tiled=True),
        lax.all_to_all(values, "sp", split_axis=2, concat_axis=1, tiled=True),
    )
    local_out = attend(query_heads[0], key_heads[0], value_heads[0], cum_gate[0])
    attended = lax.all_to_all(local_out[None], "sp", split_axis=1, concat_axis=2, tiled=True)[0]
    group_rows = attended.shape[1] // lax.axis_size("sp")
    own_rows = lax.dynamic_slice_in_dim(
        out_weight, lax.axis_index("sp") * group_rows, group_rows, 0
    )
    full_rows = lax.all_gather(own_rows, "dp", axis=1, tiled=True)
    whole_weight = lax.all_gather(full_rows, "sp", axis=0, tiled=True)
    mixed = jnp.dot(attended, whole_weight, preferred_element_type=jnp.float32)
    return mixed.astype(jnp.bfloat16)[None]


def solution(mesh):
    in_specs = (
        P("dp", "sp", None),
        P("dp", "sp", None),
        P("dp", "sp", None),
        P("dp", "sp", None),
        P(None, "dp"),
    )
    out_specs = P("dp", "sp", None)
    return jax.shard_map(body, mesh=mesh, in_specs=in_specs, out_specs=out_specs, check_vma=False)
```

```python
import functools
import math

import jax
import jax.numpy as jnp
from jax import lax
from jax.experimental import pallas as pl
from jax.experimental.pallas import tpu as pltpu
from jax.sharding import PartitionSpec as P

LANES = 128
PACK = 8
PARTS = 3
PIECES = 2
ONES = 16
MESH = pl.DeviceIdType.MESH


def ring_index(position, n):
    upper = position // (n // 2)
    return (1 - upper) * (2 * position) + upper * (2 * (n - 1 - position) + 1)


def pieces_of(columns):
    units = columns // PACK
    half = -(-units // 2)
    each = PIECES // 2
    cuts = [half * i // each for i in range(each)]
    cuts += [half + (units - half) * i // each for i in range(each + 1)]
    return [(PACK * a, PACK * (b - a)) for a, b in zip(cuts, cuts[1:])]


def fused_kernel(
    dp, depth, q, k, v, gate, w, out,
    qbuf, kbuf, vbuf, gown, gbuf, bias, qt, vt, qx, ox, lx, oin, lin, oloc, lloc, att, wg,
    load_sem, kv_send, kv_recv, gate_send, gate_recv, qx_send, qx_recv,
    ox_send, ox_recv, lx_send, lx_recv, ring_send, ring_recv, pair_send, pair_recv,
):
    tokens, width = q.shape
    columns = w.shape[0]
    pairs = width // LANES
    per_pair = LANES // depth
    own_heads = gown.shape[0]
    heads = width // depth
    both = 2 * tokens
    steps = dp // 2
    rounds = pairs // 2
    me = lax.axis_index("sp")
    mine = lax.axis_index("dp")
    core = lax.rem(me, 2)
    side_y = me // 2
    partner = me + 1 - 2 * core
    odd = lax.rem(mine, 2)
    position = (1 - odd) * (mine // 2) + odd * (dp - 1 - mine // 2)
    right = ring_index(lax.rem(position + 1, dp), dp)
    left = ring_index(lax.rem(position + dp - 1, dp), dp)
    low = side_y == 0
    high = side_y == 1

    def local(source, target, slot):
        copy = pltpu.make_async_copy(source, target, load_sem.at[slot])
        copy.start()
        return copy

    own_rows = pl.ds(pl.multiple_of(core * tokens, tokens), tokens)
    loads = [
        local(gate, gown, 0),
        local(k, kbuf.at[own_rows], 1),
        local(v, vbuf.at[own_rows], 2),
        local(q, qbuf, 3),
        local(w, wg.at[mine], 4),
    ]

    barrier = pltpu.get_barrier_semaphore()
    for d in range(1, 4):
        pl.semaphore_signal(
            barrier, inc=1, device_id=(lax.rem(me + d, 4), mine), device_id_type=MESH)

    @pl.when(core == 1)
    def _():
        for side in (left, right):
            pl.semaphore_signal(barrier, inc=1, device_id=(me, side), device_id_type=MESH)

    for copy in loads:
        copy.wait()
    gbuf[me] = gown[:, pl.ds(pl.multiple_of(side_y * both, both), both)]

    def turn(start, with_queries):
        columns_here = pl.ds(pl.multiple_of(start, tokens), tokens)

        def one(p, carry):
            lane = pl.ds(pl.multiple_of(p * LANES, LANES), LANES)
            if with_queries:
                qt[p] = jnp.transpose(qbuf[:, lane])
            vt[p, :, columns_here] = jnp.transpose(vbuf[columns_here, lane])
            return carry

        lax.fori_loop(0, pairs, one, 0)


    @pl.when(core == 0)
    def _():
        pl.semaphore_wait(barrier, 3)

    @pl.when(core == 1)
    def _():
        pl.semaphore_wait(barrier, 5)


    def remote(source, target, send, recv, device):
        return pltpu.make_async_remote_copy(
            src_ref=source, dst_ref=target, send_sem=send, recv_sem=recv,
            device_id=device, device_id_type=MESH)

    gate_copies = []
    for d in range(1, 4):
        peer = lax.rem(me + d, 4)
        gate_copies.append(remote(
            gown.at[:, pl.ds(pl.multiple_of((peer // 2) * both, both), both)],
            gbuf.at[me], gate_send.at[d - 1], gate_recv.at[d - 1], (peer, mine)))
    kv_copies = [
        remote(ref.at[own_rows], ref.at[own_rows], kv_send.at[i], kv_recv.at[i], (partner, mine))
        for i, ref in enumerate((kbuf, vbuf))
    ]

    def q_copy(p):
        return remote(
            qbuf.at[:, pl.ds(p * LANES, LANES)], qx.at[p, core],
            qx_send.at[p], qx_recv.at[p, core], (0, mine))

    for copy in gate_copies:
        copy.start()
    for copy in kv_copies:
        copy.start()

    parts = pieces_of(columns)

    def piece(owner, part):
        start, size = parts[part]
        return wg.at[owner, pl.ds(start, size)]

    def owner_of(side, step):
        shift = dp - 1 - step if side == 0 else 1 + step
        return ring_index(lax.rem(position + shift, dp), dp)

    def carries(side, step, part):
        return step < steps - 1 or (part < PIECES // 2) == (side == 0)

    def ring_copy(side, step, part):
        here = piece(owner_of(side, step - 1) if step else mine, part)
        slot = step * PIECES + part
        return remote(
            here, here, ring_send.at[side, slot], ring_recv.at[side, slot],
            (me, right if side == 0 else left))

    def pair_copy(side, step, part):
        here = piece(owner_of(side, step), part)
        slot = step * PIECES + part
        return remote(
            here, here, pair_send.at[side, slot], pair_recv.at[side, slot], (partner, mine))

    def sides_of(step):
        return range(2 if step < steps - 1 else 1)

    def ring_event(side, step, part):
        ring_copy(side, step, part).wait_recv()
        if step + 1 < steps and carries(side, step + 1, part):
            ring_copy(side, step + 1, part).start()
        pair_copy(side, step, part).start()

    every = [
        (side, step, (part + PIECES // 2 * side) % PIECES)
        for step in range(steps) for part in range(PIECES) for side in range(2)
        if carries(side, step, (part + PIECES // 2 * side) % PIECES)]

    @pl.when(core == 1)
    def _():
        for part in range(PIECES):
            for side in range(2):
                ring_copy(side, 0, (part + PIECES // 2 * side) % PIECES).start()

    @pl.when(high)
    def _():
        for p in range(pairs):
            q_copy(p).start()

    scale = depth ** -0.5 * math.log2(math.e)
    turn(core * tokens, True)
    for copy in kv_copies:
        copy.wait_recv()
    turn((1 - core) * tokens, False)
    for copy in gate_copies:
        copy.wait_recv()
    decay = jnp.concatenate([gbuf[i] for i in range(4)], axis=0) * (-(depth ** 0.5))
    rest = decay
    layers = []
    for _ in range(PARTS):
        layer = rest.astype(jnp.bfloat16).astype(jnp.float32)
        layers.append(layer)
        rest = rest - layer
    layers.append(jnp.zeros((LANES - PARTS * heads, both), jnp.float32))
    bias[...] = jnp.transpose(jnp.concatenate(layers, axis=0)).astype(jnp.bfloat16)

    bias_row = lax.broadcasted_iota(jnp.int32, (LANES, tokens), 0)
    ones = jnp.ones((ONES, both), jnp.bfloat16)

    def attend(items, keys, diagonal):
        blank = jnp.zeros((depth, tokens), jnp.bfloat16)
        logits = []
        for p, turned in items:
            lane = pl.ds(pl.multiple_of(p * LANES, LANES), LANES)
            left_side = jnp.concatenate([kbuf[0:keys, lane], bias[0:keys, :]], axis=1)
            for j in range(per_pair):
                head = p * per_pair + j
                picked = jnp.logical_and(
                    lax.rem(bias_row, heads) == head, bias_row < PARTS * heads)
                rows = [blank] * per_pair
                rows[j] = turned[j * depth:(j + 1) * depth, :]
                right_side = jnp.concatenate(
                    rows + [jnp.where(picked, 1.0, 0.0).astype(jnp.bfloat16)], axis=0)
                logits.append(
                    jnp.dot(left_side, right_side, preferred_element_type=jnp.float32))
        if diagonal:
            first = keys - tokens
            allowed = (
                lax.broadcasted_iota(jnp.int32, (tokens, tokens), 0)
                <= lax.broadcasted_iota(jnp.int32, (tokens, tokens), 1))
            for n, plain in enumerate(logits):
                last = jnp.where(allowed, plain[first:, :], -jnp.inf)
                logits[n] = jnp.concatenate([plain[:first, :], last], axis=0) if first else last
        tops = [jnp.max(x, axis=0, keepdims=True) for x in logits]
        scores = [
            jnp.exp2((x - top) * scale).astype(jnp.bfloat16) for x, top in zip(logits, tops)]
        results = []
        for i, (p, _) in enumerate(items):
            found = []
            for j in range(per_pair):
                n = i * per_pair + j
                weights = jnp.concatenate(
                    [vt[p, j * depth:(j + 1) * depth, 0:keys], ones[:, 0:keys]], axis=0)
                summed = jnp.dot(weights, scores[n], preferred_element_type=jnp.float32)
                total = summed[depth:depth + 1, :]
                found.append(
                    (summed[:depth, :] * (1.0 / total), tops[n] * scale + jnp.log2(total)))
            results.append(found)
        return results

    def own_pairs(first, last, keys):
        span = range(first, last)
        results = attend([(p, qt[p]) for p in span], keys, True)

        @pl.when(low)
        def _():
            for p, found in zip(span, results):
                for j in range(per_pair):
                    att[p, j * depth:(j + 1) * depth, :] = found[j][0].astype(jnp.bfloat16)

        @pl.when(high)
        def _():
            for p, found in zip(span, results):
                for j in range(per_pair):
                    oloc[p, j * depth:(j + 1) * depth, :] = found[j][0]
                    lloc[p, j:j + 1, :] = found[j][1]

    def o_copy(p, block):
        return remote(
            ox.at[p, block], oin.at[p], ox_send.at[p, block], ox_recv.at[p], (2 + block, mine))

    def l_copy(p, block):
        return remote(
            lx.at[p, block], lin.at[p], lx_send.at[p, block], lx_recv.at[p], (2 + block, mine))

    def other_pair(p):
        for block in range(2):
            remote(
                qbuf.at[:, pl.ds(0, LANES)], qx.at[p, block],
                qx_send.at[p], qx_recv.at[p, block], (partner, mine)).wait_recv()
        results = attend([(p, jnp.transpose(qx[p, block])) for block in range(2)], both, False)
        for block in range(2):
            for j in range(per_pair):
                found = results[block][j]
                ox[p, block, j * depth:(j + 1) * depth, :] = found[0].astype(jnp.bfloat16)
                lx[p, block, j:j + 1, :] = found[1]
            o_copy(p, block).start()
            l_copy(p, block).start()

    def merge(p, carry):
        o_copy(p, 0).wait_recv()
        l_copy(p, 0).wait_recv()
        for j in range(per_pair):
            rows = pl.ds(j * depth, depth)
            near, far = lloc[p, j:j + 1, :], lin[p, j:j + 1, :]
            top = jnp.maximum(near, far)
            near, far = jnp.exp2(near - top), jnp.exp2(far - top)
            inverse = 1.0 / (near + far)
            mixed = oloc[p, rows, :] * (near * inverse) + oin[p, rows, :].astype(jnp.float32) * (far * inverse)
            att[p, rows, :] = mixed.astype(jnp.bfloat16)
        return carry

    def project(owner):
        total = jnp.dot(
            wg[owner], att[...].reshape(width, tokens), preferred_element_type=jnp.float32)
        out[pl.ds(pl.multiple_of(owner * columns, PACK), columns), :] = total.astype(jnp.bfloat16)

    def merge_to(first, last):
        @pl.when(high)
        def _():
            lax.fori_loop(first, last, merge, 0)

    def finish(step):
        for side in sides_of(step):
            project(owner_of(side, step))

    @pl.when(core == 0)
    def _():
        for r in range(rounds):
            own_pairs(r * pairs // rounds, (r + 1) * pairs // rounds, tokens)

        @pl.when(low)
        def _():
            for p in range(pairs):
                other_pair(p)

        merge_to(0, pairs)
        project(mine)
        for step in range(steps):
            for key in every:
                if key[1] == step:
                    pair_copy(*key).wait_recv()
            finish(step)

        @pl.when(low)
        def _():
            for p in range(pairs):
                for block in range(2):
                    o_copy(p, block).wait_send()
                    l_copy(p, block).wait_send()

    @pl.when(core == 1)
    def _():
        todo = list(every)

        def advance(count):
            for _ in range(count):
                ring_event(*todo.pop(0))

        for r in range(rounds):
            own_pairs(r * pairs // rounds, (r + 1) * pairs // rounds, both)
            advance(2)
        while todo and todo[0][1] < steps - 1:
            advance(1)
        merge_to(0, pairs)
        project(mine)
        for step in range(steps - 1):
            finish(step)
        advance(len(todo))
        finish(steps - 1)
        for key in every:
            ring_copy(*key).wait_send()
            pair_copy(*key).wait_send()

    for copy in gate_copies + kv_copies:
        copy.wait_send()

    @pl.when(high)
    def _():
        for p in range(pairs):
            q_copy(p).wait_send()


def fused(dp, depth, q, k, v, gate, w):
    tokens, width = q.shape
    columns = w.shape[0]
    pairs = width // LANES
    both = 2 * tokens
    steps = dp // 2
    slots = steps * PIECES
    any_spec = pl.BlockSpec(memory_space=pl.ANY)
    dma = pltpu.SemaphoreType.DMA
    low, wide = jnp.bfloat16, jnp.float32
    per_pair = LANES // depth
    return pl.pallas_call(
        functools.partial(fused_kernel, dp, depth),
        out_shape=pltpu.VMEM((columns * dp, tokens), low),
        in_specs=[any_spec] * 5,
        out_specs=pl.BlockSpec(memory_space=pltpu.VMEM),
        scratch_shapes=[
            pltpu.VMEM((tokens, width), low),
            pltpu.VMEM((both, width), low),
            pltpu.VMEM((both, width), low),
            pltpu.VMEM(gate.shape, wide),
            pltpu.VMEM((4, gate.shape[0], both), wide),
            pltpu.VMEM((both, LANES), low),
            pltpu.VMEM((pairs, LANES, tokens), low),
            pltpu.VMEM((pairs, LANES, both), low),
            pltpu.VMEM((pairs, 2, tokens, LANES), low),
            pltpu.VMEM((pairs, 2, LANES, tokens), low),
            pltpu.VMEM((pairs, 2, per_pair, tokens), wide),
            pltpu.VMEM((pairs, LANES, tokens), low),
            pltpu.VMEM((pairs, per_pair, tokens), wide),
            pltpu.VMEM((pairs, LANES, tokens), wide),
            pltpu.VMEM((pairs, per_pair, tokens), wide),
            pltpu.VMEM((pairs, LANES, tokens), low),
            pltpu.VMEM((dp, columns, width), low),
            dma((5,)), dma((2,)), dma((2,)), dma((3,)), dma((3,)),
            dma((pairs,)), dma((pairs, 2)),
            dma((pairs, 2)), dma((pairs,)), dma((pairs, 2)), dma((pairs,)),
            dma((2, slots)), dma((2, slots)), dma((2, slots)), dma((2, slots)),
        ],
        compiler_params=pltpu.CompilerParams(
            collective_id=0, has_side_effects=True, vmem_limit_bytes=48 * 1024 * 1024),
    )(*(pltpu.with_memory_space_constraint(x, pltpu.HBM) for x in (q, k, v, gate, w)))


def fits(sp, dp, tokens, width, depth, columns, own_heads):
    return (
        sp == 4 and dp % 2 == 0 and dp >= 4
        and tokens <= 256 and tokens % LANES == 0 and LANES % depth == 0 and depth % 16 == 0
        and width % (2 * LANES) == 0 and columns % PACK == 0 and columns >= PIECES * PACK
        and own_heads * sp * depth == width and PARTS * own_heads * sp <= LANES
        and width == 8 * LANES and dp == 8
    )


def attend(query_all, key_all, value_all, gate_all):
    length, width = query_all.shape
    heads = gate_all.shape[0]
    depth = width // heads
    block_rows = min(512, length)
    block_count = length // block_rows
    score_scale = depth ** (-0.5)
    query_blocks = query_all.reshape(block_count, block_rows, heads, depth)
    key_blocks = key_all.reshape(block_count, block_rows, heads, depth)
    value_blocks = value_all.reshape(block_count, block_rows, heads, depth)
    gate_blocks = gate_all.reshape(heads, block_count, block_rows).transpose(1, 0, 2)
    offsets = jnp.arange(block_rows, dtype=jnp.int32)

    def one_block(block_index):
        query_part = lax.dynamic_index_in_dim(query_blocks, block_index, 0, keepdims=False)
        gate_part = lax.dynamic_index_in_dim(gate_blocks, block_index, 0, keepdims=False)
        query_rows = block_index * block_rows + offsets

        def key_step(key_block, carry):
            running_max, running_sum, weighted = carry
            key_part = lax.dynamic_index_in_dim(key_blocks, key_block, 0, keepdims=False)
            value_part = lax.dynamic_index_in_dim(value_blocks, key_block, 0, keepdims=False)
            gate_keys = lax.dynamic_index_in_dim(gate_blocks, key_block, 0, keepdims=False)
            logits = (
                jnp.einsum("qhe,khe->hqk", query_part, key_part, preferred_element_type=jnp.float32)
                * score_scale
            )
            logits = logits + gate_part[:, :, None] - gate_keys[:, None, :]
            key_rows = key_block * block_rows + offsets
            allowed = key_rows[None, :] <= query_rows[:, None]
            logits = jnp.where(allowed[None], logits, -jnp.inf)
            new_max = jnp.maximum(running_max, jnp.max(logits, axis=-1))
            scores = jnp.exp(logits - new_max[..., None])
            factor = jnp.exp(running_max - new_max)
            running_sum = running_sum * factor + jnp.sum(scores, axis=-1)
            weighted = weighted * factor[..., None] + jnp.einsum(
                "hqk,khe->hqe",
                scores.astype(jnp.bfloat16),
                value_part,
                preferred_element_type=jnp.float32,
            )
            return (new_max, running_sum, weighted)

        start_state = (
            jnp.full((heads, block_rows), -jnp.inf, jnp.float32),
            jnp.zeros((heads, block_rows), jnp.float32),
            jnp.zeros((heads, block_rows, depth), jnp.float32),
        )
        final_max, final_sum, weighted = lax.fori_loop(0, block_index + 1, key_step, start_state)
        result = weighted / final_sum[..., None]
        return result.transpose(1, 0, 2).astype(jnp.bfloat16)

    outputs = lax.map(one_block, jnp.arange(block_count, dtype=jnp.int32))
    return outputs.reshape(length, width)


def body(queries, keys, values, cum_gate, out_weight):
    sp, dp = lax.axis_size("sp"), lax.axis_size("dp")
    tokens, width = queries.shape[1:]
    depth = width // (cum_gate.shape[1] * sp)
    if fits(sp, dp, tokens, width, depth, out_weight.shape[1], cum_gate.shape[1]):
        mixed = fused(dp, depth, queries[0], keys[0], values[0], cum_gate[0], out_weight.T)
        return mixed.T[None]
    query_heads, key_heads, value_heads = (
        lax.all_to_all(queries, "sp", split_axis=2, concat_axis=1, tiled=True),
        lax.all_to_all(keys, "sp", split_axis=2, concat_axis=1, tiled=True),
        lax.all_to_all(values, "sp", split_axis=2, concat_axis=1, tiled=True),
    )
    local_out = attend(query_heads[0], key_heads[0], value_heads[0], cum_gate[0])
    attended = lax.all_to_all(local_out[None], "sp", split_axis=1, concat_axis=2, tiled=True)[0]
    group_rows = attended.shape[1] // lax.axis_size("sp")
    own_rows = lax.dynamic_slice_in_dim(
        out_weight, lax.axis_index("sp") * group_rows, group_rows, 0
    )
    full_rows = lax.all_gather(own_rows, "dp", axis=1, tiled=True)
    whole_weight = lax.all_gather(full_rows, "sp", axis=0, tiled=True)
    mixed = jnp.dot(attended, whole_weight, preferred_element_type=jnp.float32)
    return mixed.astype(jnp.bfloat16)[None]


def solution(mesh):
    in_specs = (
        P("dp", "sp", None),
        P("dp", "sp", None),
        P("dp", "sp", None),
        P("dp", "sp", None),
        P(None, "dp"),
    )
    out_specs = P("dp", "sp", None)
    return jax.shard_map(body, mesh=mesh, in_specs=in_specs, out_specs=out_specs, check_vma=False)
```

```python
import functools
import math

import jax
import jax.numpy as jnp
from jax import lax
from jax.experimental import pallas as pl
from jax.experimental.pallas import tpu as pltpu
from jax.sharding import PartitionSpec as P

LANES = 128
PACK = 8
PARTS = 3
PIECES = 2
LARGE = 3
ONES = 16
MESH = pl.DeviceIdType.MESH


def ring_index(position, n):
    upper = position // (n // 2)
    return (1 - upper) * (2 * position) + upper * (2 * (n - 1 - position) + 1)


def pieces_of(columns):
    units = columns // PACK
    half = -(-units // 2)
    each = PIECES // 2
    cuts = [half * i // each for i in range(each)]
    cuts += [half + (units - half) * i // each for i in range(each + 1)]
    return [(PACK * a, PACK * (b - a)) for a, b in zip(cuts, cuts[1:])]


def fused_kernel(
    dp, depth, q, k, v, gate, w, out,
    qbuf, kbuf, vbuf, gown, gbuf, bias, qt, vt, qx, ox, lx, oin, lin, oloc, lloc, att, wg,
    load_sem, kv_send, kv_recv, gate_send, gate_recv, qx_send, qx_recv,
    ox_send, ox_recv, lx_send, lx_recv, ring_send, ring_recv, pair_send, pair_recv,
):
    tokens, width = q.shape
    columns = w.shape[0]
    pairs = width // LANES
    per_pair = LANES // depth
    own_heads = gown.shape[0]
    heads = width // depth
    both = 2 * tokens
    steps = dp // 2
    rounds = pairs // 2
    me = lax.axis_index("sp")
    mine = lax.axis_index("dp")
    core = lax.rem(me, 2)
    side_y = me // 2
    partner = me + 1 - 2 * core
    odd = lax.rem(mine, 2)
    position = (1 - odd) * (mine // 2) + odd * (dp - 1 - mine // 2)
    right = ring_index(lax.rem(position + 1, dp), dp)
    left = ring_index(lax.rem(position + dp - 1, dp), dp)
    low = side_y == 0
    high = side_y == 1

    def local(source, target, slot):
        copy = pltpu.make_async_copy(source, target, load_sem.at[slot])
        copy.start()
        return copy

    own_rows = pl.ds(pl.multiple_of(core * tokens, tokens), tokens)
    loads = [
        local(gate, gown, 0),
        local(k, kbuf.at[own_rows], 1),
        local(v, vbuf.at[own_rows], 2),
        local(q, qbuf, 3),
        local(w, wg.at[mine], 4),
    ]

    barrier = pltpu.get_barrier_semaphore()
    for d in range(1, 4):
        pl.semaphore_signal(
            barrier, inc=1, device_id=(lax.rem(me + d, 4), mine), device_id_type=MESH)

    @pl.when(core == 1)
    def _():
        for side in (left, right):
            pl.semaphore_signal(barrier, inc=1, device_id=(me, side), device_id_type=MESH)

    for copy in loads:
        copy.wait()
    gbuf[me] = gown[:, pl.ds(pl.multiple_of(side_y * both, both), both)]

    def turn(start, with_queries):
        columns_here = pl.ds(pl.multiple_of(start, tokens), tokens)

        def one(p, carry):
            lane = pl.ds(pl.multiple_of(p * LANES, LANES), LANES)
            if with_queries:
                qt[p] = jnp.transpose(qbuf[:, lane])
            vt[p, :, columns_here] = jnp.transpose(vbuf[columns_here, lane])
            return carry

        lax.fori_loop(0, pairs, one, 0)


    @pl.when(core == 0)
    def _():
        pl.semaphore_wait(barrier, 3)

    @pl.when(core == 1)
    def _():
        pl.semaphore_wait(barrier, 5)


    def remote(source, target, send, recv, device):
        return pltpu.make_async_remote_copy(
            src_ref=source, dst_ref=target, send_sem=send, recv_sem=recv,
            device_id=device, device_id_type=MESH)

    gate_copies = []
    for d in range(1, 4):
        peer = lax.rem(me + d, 4)
        gate_copies.append(remote(
            gown.at[:, pl.ds(pl.multiple_of((peer // 2) * both, both), both)],
            gbuf.at[me], gate_send.at[d - 1], gate_recv.at[d - 1], (peer, mine)))
    kv_copies = [
        remote(ref.at[own_rows], ref.at[own_rows], kv_send.at[i], kv_recv.at[i], (partner, mine))
        for i, ref in enumerate((kbuf, vbuf))
    ]

    def q_copy(p):
        return remote(
            qbuf.at[:, pl.ds(p * LANES, LANES)], qx.at[p, core],
            qx_send.at[p], qx_recv.at[p, core], (0, mine))

    for copy in gate_copies:
        copy.start()
    for copy in kv_copies:
        copy.start()

    parts = pieces_of(columns)
    final = []
    for start, size in parts:
        large = size * LARGE // 4 // PACK * PACK
        final += [(start, large), (start + large, size - large)]

    def piece(owner, step, part):
        start, size = (parts if step < steps - 1 else final)[part]
        return wg.at[owner, pl.ds(start, size)]

    def owner_of(side, step):
        shift = dp - 1 - step if side == 0 else 1 + step
        return ring_index(lax.rem(position + shift, dp), dp)

    def carries(side, step, part):
        return step < steps - 1 or (part < PIECES) == (side == 0)

    def ring_copy(side, step, part):
        here = piece(owner_of(side, step - 1) if step else mine, step, part)
        slot = step * PIECES + part
        return remote(
            here, here, ring_send.at[side, slot], ring_recv.at[side, slot],
            (me, right if side == 0 else left))

    def pair_copy(side, step, part):
        here = piece(owner_of(side, step), step, part)
        slot = step * PIECES + part
        return remote(
            here, here, pair_send.at[side, slot], pair_recv.at[side, slot], (partner, mine))

    def sides_of(step):
        return range(2 if step < steps - 1 else 1)

    def ring_event(side, step, part):
        ring_copy(side, step, part).wait_recv()
        if step + 2 < steps:
            ring_copy(side, step + 1, part).start()
        elif step + 1 < steps:
            for smaller in (2 * part, 2 * part + 1):
                if carries(side, step + 1, smaller):
                    ring_copy(side, step + 1, smaller).start()
        pair_copy(side, step, part).start()

    every = [
        (side, step, (part + PIECES // 2 * side) % PIECES)
        for step in range(steps - 1) for part in range(PIECES) for side in range(2)]
    every += [(side, steps - 1, part + PIECES * side) for part in range(PIECES) for side in range(2)]

    @pl.when(core == 1)
    def _():
        for part in range(PIECES):
            for side in range(2):
                ring_copy(side, 0, (part + PIECES // 2 * side) % PIECES).start()

    @pl.when(high)
    def _():
        for p in range(pairs):
            q_copy(p).start()

    scale = depth ** -0.5 * math.log2(math.e)
    turn(core * tokens, True)
    for copy in kv_copies:
        copy.wait_recv()
    turn((1 - core) * tokens, False)
    for copy in gate_copies:
        copy.wait_recv()
    decay = jnp.concatenate([gbuf[i] for i in range(4)], axis=0) * (-(depth ** 0.5))
    rest = decay
    layers = []
    for _ in range(PARTS):
        layer = rest.astype(jnp.bfloat16).astype(jnp.float32)
        layers.append(layer)
        rest = rest - layer
    layers.append(jnp.zeros((LANES - PARTS * heads, both), jnp.float32))
    bias[...] = jnp.transpose(jnp.concatenate(layers, axis=0)).astype(jnp.bfloat16)

    bias_row = lax.broadcasted_iota(jnp.int32, (LANES, tokens), 0)
    ones = jnp.ones((ONES, both), jnp.bfloat16)

    def attend(items, keys, diagonal):
        blank = jnp.zeros((depth, tokens), jnp.bfloat16)
        logits = []
        for p, turned in items:
            lane = pl.ds(pl.multiple_of(p * LANES, LANES), LANES)
            left_side = jnp.concatenate([kbuf[0:keys, lane], bias[0:keys, :]], axis=1)
            for j in range(per_pair):
                head = p * per_pair + j
                picked = jnp.logical_and(
                    lax.rem(bias_row, heads) == head, bias_row < PARTS * heads)
                rows = [blank] * per_pair
                rows[j] = turned[j * depth:(j + 1) * depth, :]
                right_side = jnp.concatenate(
                    rows + [jnp.where(picked, 1.0, 0.0).astype(jnp.bfloat16)], axis=0)
                logits.append(
                    jnp.dot(left_side, right_side, preferred_element_type=jnp.float32))
        if diagonal:
            first = keys - tokens
            allowed = (
                lax.broadcasted_iota(jnp.int32, (tokens, tokens), 0)
                <= lax.broadcasted_iota(jnp.int32, (tokens, tokens), 1))
            for n, plain in enumerate(logits):
                last = jnp.where(allowed, plain[first:, :], -jnp.inf)
                logits[n] = jnp.concatenate([plain[:first, :], last], axis=0) if first else last
        tops = [jnp.max(x, axis=0, keepdims=True) for x in logits]
        scores = [
            jnp.exp2((x - top) * scale).astype(jnp.bfloat16) for x, top in zip(logits, tops)]
        results = []
        for i, (p, _) in enumerate(items):
            found = []
            for j in range(per_pair):
                n = i * per_pair + j
                weights = jnp.concatenate(
                    [vt[p, j * depth:(j + 1) * depth, 0:keys], ones[:, 0:keys]], axis=0)
                summed = jnp.dot(weights, scores[n], preferred_element_type=jnp.float32)
                total = summed[depth:depth + 1, :]
                found.append(
                    (summed[:depth, :] * (1.0 / total), tops[n] * scale + jnp.log2(total)))
            results.append(found)
        return results

    def own_pairs(first, last, keys):
        span = range(first, last)
        results = attend([(p, qt[p]) for p in span], keys, True)

        @pl.when(low)
        def _():
            for p, found in zip(span, results):
                for j in range(per_pair):
                    att[p, j * depth:(j + 1) * depth, :] = found[j][0].astype(jnp.bfloat16)

        @pl.when(high)
        def _():
            for p, found in zip(span, results):
                for j in range(per_pair):
                    oloc[p, j * depth:(j + 1) * depth, :] = found[j][0]
                    lloc[p, j:j + 1, :] = found[j][1]

    def o_copy(p, block):
        return remote(
            ox.at[p, block], oin.at[p], ox_send.at[p, block], ox_recv.at[p], (2 + block, mine))

    def l_copy(p, block):
        return remote(
            lx.at[p, block], lin.at[p], lx_send.at[p, block], lx_recv.at[p], (2 + block, mine))

    def other_pair(p):
        for block in range(2):
            remote(
                qbuf.at[:, pl.ds(0, LANES)], qx.at[p, block],
                qx_send.at[p], qx_recv.at[p, block], (partner, mine)).wait_recv()
        results = attend([(p, jnp.transpose(qx[p, block])) for block in range(2)], both, False)
        for block in range(2):
            for j in range(per_pair):
                found = results[block][j]
                ox[p, block, j * depth:(j + 1) * depth, :] = found[0].astype(jnp.bfloat16)
                lx[p, block, j:j + 1, :] = found[1]
            o_copy(p, block).start()
            l_copy(p, block).start()

    def merge(p, carry):
        o_copy(p, 0).wait_recv()
        l_copy(p, 0).wait_recv()
        for j in range(per_pair):
            rows = pl.ds(j * depth, depth)
            near, far = lloc[p, j:j + 1, :], lin[p, j:j + 1, :]
            top = jnp.maximum(near, far)
            near, far = jnp.exp2(near - top), jnp.exp2(far - top)
            inverse = 1.0 / (near + far)
            mixed = oloc[p, rows, :] * (near * inverse) + oin[p, rows, :].astype(jnp.float32) * (far * inverse)
            att[p, rows, :] = mixed.astype(jnp.bfloat16)
        return carry

    def project(owner):
        total = jnp.dot(
            wg[owner], att[...].reshape(width, tokens), preferred_element_type=jnp.float32)
        out[pl.ds(pl.multiple_of(owner * columns, PACK), columns), :] = total.astype(jnp.bfloat16)

    def merge_to(first, last):
        @pl.when(high)
        def _():
            lax.fori_loop(first, last, merge, 0)

    def finish(step):
        for side in sides_of(step):
            project(owner_of(side, step))

    @pl.when(core == 0)
    def _():
        for r in range(rounds):
            own_pairs(r * pairs // rounds, (r + 1) * pairs // rounds, tokens)

        @pl.when(low)
        def _():
            for p in range(pairs):
                other_pair(p)

        merge_to(0, pairs)
        project(mine)
        for step in range(steps):
            for key in every:
                if key[1] == step:
                    pair_copy(*key).wait_recv()
            finish(step)

        @pl.when(low)
        def _():
            for p in range(pairs):
                for block in range(2):
                    o_copy(p, block).wait_send()
                    l_copy(p, block).wait_send()

    @pl.when(core == 1)
    def _():
        todo = list(every)

        def advance(count):
            for _ in range(count):
                ring_event(*todo.pop(0))

        for r in range(rounds):
            own_pairs(r * pairs // rounds, (r + 1) * pairs // rounds, both)
            advance(2)
        while todo and todo[0][1] < steps - 1:
            advance(1)
        merge_to(0, pairs)
        project(mine)
        for step in range(steps - 1):
            finish(step)
        advance(len(todo))
        finish(steps - 1)
        for key in every:
            ring_copy(*key).wait_send()
            pair_copy(*key).wait_send()

    for copy in gate_copies + kv_copies:
        copy.wait_send()

    @pl.when(high)
    def _():
        for p in range(pairs):
            q_copy(p).wait_send()


def fused(dp, depth, q, k, v, gate, w):
    tokens, width = q.shape
    columns = w.shape[0]
    pairs = width // LANES
    both = 2 * tokens
    steps = dp // 2
    slots = (steps + 1) * PIECES
    any_spec = pl.BlockSpec(memory_space=pl.ANY)
    dma = pltpu.SemaphoreType.DMA
    low, wide = jnp.bfloat16, jnp.float32
    per_pair = LANES // depth
    return pl.pallas_call(
        functools.partial(fused_kernel, dp, depth),
        out_shape=pltpu.VMEM((columns * dp, tokens), low),
        in_specs=[any_spec] * 5,
        out_specs=pl.BlockSpec(memory_space=pltpu.VMEM),
        scratch_shapes=[
            pltpu.VMEM((tokens, width), low),
            pltpu.VMEM((both, width), low),
            pltpu.VMEM((both, width), low),
            pltpu.VMEM(gate.shape, wide),
            pltpu.VMEM((4, gate.shape[0], both), wide),
            pltpu.VMEM((both, LANES), low),
            pltpu.VMEM((pairs, LANES, tokens), low),
            pltpu.VMEM((pairs, LANES, both), low),
            pltpu.VMEM((pairs, 2, tokens, LANES), low),
            pltpu.VMEM((pairs, 2, LANES, tokens), low),
            pltpu.VMEM((pairs, 2, per_pair, tokens), wide),
            pltpu.VMEM((pairs, LANES, tokens), low),
            pltpu.VMEM((pairs, per_pair, tokens), wide),
            pltpu.VMEM((pairs, LANES, tokens), wide),
            pltpu.VMEM((pairs, per_pair, tokens), wide),
            pltpu.VMEM((pairs, LANES, tokens), low),
            pltpu.VMEM((dp, columns, width), low),
            dma((5,)), dma((2,)), dma((2,)), dma((3,)), dma((3,)),
            dma((pairs,)), dma((pairs, 2)),
            dma((pairs, 2)), dma((pairs,)), dma((pairs, 2)), dma((pairs,)),
            dma((2, slots)), dma((2, slots)), dma((2, slots)), dma((2, slots)),
        ],
        compiler_params=pltpu.CompilerParams(
            collective_id=0, has_side_effects=True, vmem_limit_bytes=48 * 1024 * 1024),
    )(*(pltpu.with_memory_space_constraint(x, pltpu.HBM) for x in (q, k, v, gate, w)))


def fits(sp, dp, tokens, width, depth, columns, own_heads):
    return (
        sp == 4 and dp % 2 == 0 and dp >= 4
        and tokens <= 256 and tokens % LANES == 0 and LANES % depth == 0 and depth % 16 == 0
        and width % (2 * LANES) == 0 and columns % PACK == 0 and columns >= PIECES * PACK
        and own_heads * sp * depth == width and PARTS * own_heads * sp <= LANES
        and width == 8 * LANES and dp == 8
    )


def attend(query_all, key_all, value_all, gate_all):
    length, width = query_all.shape
    heads = gate_all.shape[0]
    depth = width // heads
    block_rows = min(512, length)
    block_count = length // block_rows
    score_scale = depth ** (-0.5)
    query_blocks = query_all.reshape(block_count, block_rows, heads, depth)
    key_blocks = key_all.reshape(block_count, block_rows, heads, depth)
    value_blocks = value_all.reshape(block_count, block_rows, heads, depth)
    gate_blocks = gate_all.reshape(heads, block_count, block_rows).transpose(1, 0, 2)
    offsets = jnp.arange(block_rows, dtype=jnp.int32)

    def one_block(block_index):
        query_part = lax.dynamic_index_in_dim(query_blocks, block_index, 0, keepdims=False)
        gate_part = lax.dynamic_index_in_dim(gate_blocks, block_index, 0, keepdims=False)
        query_rows = block_index * block_rows + offsets

        def key_step(key_block, carry):
            running_max, running_sum, weighted = carry
            key_part = lax.dynamic_index_in_dim(key_blocks, key_block, 0, keepdims=False)
            value_part = lax.dynamic_index_in_dim(value_blocks, key_block, 0, keepdims=False)
            gate_keys = lax.dynamic_index_in_dim(gate_blocks, key_block, 0, keepdims=False)
            logits = (
                jnp.einsum("qhe,khe->hqk", query_part, key_part, preferred_element_type=jnp.float32)
                * score_scale
            )
            logits = logits + gate_part[:, :, None] - gate_keys[:, None, :]
            key_rows = key_block * block_rows + offsets
            allowed = key_rows[None, :] <= query_rows[:, None]
            logits = jnp.where(allowed[None], logits, -jnp.inf)
            new_max = jnp.maximum(running_max, jnp.max(logits, axis=-1))
            scores = jnp.exp(logits - new_max[..., None])
            factor = jnp.exp(running_max - new_max)
            running_sum = running_sum * factor + jnp.sum(scores, axis=-1)
            weighted = weighted * factor[..., None] + jnp.einsum(
                "hqk,khe->hqe",
                scores.astype(jnp.bfloat16),
                value_part,
                preferred_element_type=jnp.float32,
            )
            return (new_max, running_sum, weighted)

        start_state = (
            jnp.full((heads, block_rows), -jnp.inf, jnp.float32),
            jnp.zeros((heads, block_rows), jnp.float32),
            jnp.zeros((heads, block_rows, depth), jnp.float32),
        )
        final_max, final_sum, weighted = lax.fori_loop(0, block_index + 1, key_step, start_state)
        result = weighted / final_sum[..., None]
        return result.transpose(1, 0, 2).astype(jnp.bfloat16)

    outputs = lax.map(one_block, jnp.arange(block_count, dtype=jnp.int32))
    return outputs.reshape(length, width)


def body(queries, keys, values, cum_gate, out_weight):
    sp, dp = lax.axis_size("sp"), lax.axis_size("dp")
    tokens, width = queries.shape[1:]
    depth = width // (cum_gate.shape[1] * sp)
    if fits(sp, dp, tokens, width, depth, out_weight.shape[1], cum_gate.shape[1]):
        mixed = fused(dp, depth, queries[0], keys[0], values[0], cum_gate[0], out_weight.T)
        return mixed.T[None]
    query_heads, key_heads, value_heads = (
        lax.all_to_all(queries, "sp", split_axis=2, concat_axis=1, tiled=True),
        lax.all_to_all(keys, "sp", split_axis=2, concat_axis=1, tiled=True),
        lax.all_to_all(values, "sp", split_axis=2, concat_axis=1, tiled=True),
    )
    local_out = attend(query_heads[0], key_heads[0], value_heads[0], cum_gate[0])
    attended = lax.all_to_all(local_out[None], "sp", split_axis=1, concat_axis=2, tiled=True)[0]
    group_rows = attended.shape[1] // lax.axis_size("sp")
    own_rows = lax.dynamic_slice_in_dim(
        out_weight, lax.axis_index("sp") * group_rows, group_rows, 0
    )
    full_rows = lax.all_gather(own_rows, "dp", axis=1, tiled=True)
    whole_weight = lax.all_gather(full_rows, "sp", axis=0, tiled=True)
    mixed = jnp.dot(attended, whole_weight, preferred_element_type=jnp.float32)
    return mixed.astype(jnp.bfloat16)[None]


def solution(mesh):
    in_specs = (
        P("dp", "sp", None),
        P("dp", "sp", None),
        P("dp", "sp", None),
        P("dp", "sp", None),
        P(None, "dp"),
    )
    out_specs = P("dp", "sp", None)
    return jax.shard_map(body, mesh=mesh, in_specs=in_specs, out_specs=out_specs, check_vma=False)
```
